256 devices in a mesh: ep: 64 (over z, x, core), tp: 4 (over y).
Axes of the slice: x: 4, y: 4, z: 8, core: 2. Of those that a mesh axis runs over, the one named last changes fastest.
Arguments:
- head_inputs_unfiltered: bfloat16 [8192, 4096], P('ep', 'tp'), may hold values from -6 to 6
- group_write_vectors: bfloat16 [8192, 512], P('ep', 'tp'), may hold values from -6 to 6
- group_read_vectors: bfloat16 [8192, 512], P('ep', 'tp'), may hold values from -6 to 6
- output_gate_inputs: bfloat16 [8192, 4096], P('ep', 'tp'), may hold values from -6 to 6
- step_preactivation: float32 [64, 8192], P('tp', 'ep'), may hold values from -3.2 to 3.6
- extra_decay_logs: float32 [64, 8192], P('tp', 'ep'), may hold values from -0.7 to 0
- head_decay_logs: float32 [64], P('tp'), may hold values from -16 to -2.7
- head_filter_taps: bfloat16 [4, 4096], P(None, 'tp'), may hold values from -3 to 3
- write_filter_taps: bfloat16 [4, 512], P(None, 'tp'), may hold values from -3 to 3
- read_filter_taps: bfloat16 [4, 512], P(None, 'tp'), may hold values from -3 to 3
- grouped_norm_gain: float32 [4096], P('tp'), may hold values from 0.1 to 1.9
- mixer_output_weight: bfloat16 [4096, 2048], P('tp'), may hold values from -0.09375 to 0.09375
- expert_input_rows: bfloat16 [32768, 2048], P(('ep', 'tp')), may hold values from -6 to 6
- expert_norm_gain: float32 [2048], replicated, may hold values from 0.1 to 1.9
- routes: int32 [32768, 2], P(('ep', 'tp')), may hold values from 0 to 63, all different within a row; in each aligned block of 128 rows (0 to 127, 128 to 255, ...) at most 6 rows name the same one
- router_chosen_scores: bfloat16 [32768, 2], P(('ep', 'tp')), may hold values from 0.049804688 to 1
- routed_gate_weight: bfloat16 [64, 2048, 1024], P('ep', None, 'tp'), may hold values from -0.125 to 0.125
- routed_up_weight: bfloat16 [64, 2048, 1024], P('ep', None, 'tp'), may hold values from -0.125 to 0.125
- routed_down_weight: bfloat16 [64, 1024, 2048], P('ep', 'tp'), may hold values from -0.1875 to 0.1875
- shared_gate_weight: bfloat16 [2048, 512], P(None, 'tp'), may hold values from -0.125 to 0.125
- shared_up_weight: bfloat16 [2048, 512], P(None, 'tp'), may hold values from -0.125 to 0.125
- shared_down_weight: bfloat16 [512, 2048], P('tp'), may hold values from -0.25 to 0.25
Outputs:
- mixer_result: bfloat16 [8192, 2048], P(('ep', 'tp'))
- moe_result: bfloat16 [32768, 2048], P(('ep', 'tp'))
The draws below stay inside these ranges and needn't reach their ends.
Inputs may be any that keep to these rules, and one draw needn't show every extreme that they name: `routes`: within the 128 rows of one device no expert is named more than 6 times; a row names 2 different experts.
All inputs are finite; a program needn't handle non-finite values.
Results may differ from the reference program's by a relative error of at most 0.0095.
Values may be sent and summed in bfloat16 or wider, within the bound.
No kernel may reach another device: no remote copies, remote signals or barrier semaphores. Data moves between devices by JAX's collectives and lax.ppermute only.
A program may use at most 128 MiB of HBM per device.

```python
import math
import jax
import jax.numpy as jnp
import numpy as np
from jax import lax

D = 2048
HEADS = 64
HEAD_DIM = 64
GROUPS = 4
STATE = 128
CONV = 4
BLOCK = 64
INNER = 4096
MIX_ROWS = 128
MIX_TOKENS = 8192
EXPERT_FF = 1024
SHARED_FF = 512
EXPERTS = 64
TOP_K = 2
MOE_ROWS = 128
MOE_TOKENS = 32768
CAPACITY = 6
N_TP = 4


def draw_step_preactivation(key, part):
    key_noise, key_shift = jax.random.split(key)
    block_total = MIX_TOKENS // MIX_ROWS
    noise = jnp.clip(0.7 * jax.random.normal(key_noise, (HEADS, MIX_TOKENS), jnp.float32), -1.6, 1.6)
    shifts = jax.random.uniform(key_shift, (block_total,), jnp.float32, -1.0, 1.5)
    return noise + jnp.repeat(shifts, MIX_ROWS)[None, :]


def draw_extra_decay_logs(key, part):
    key_place, key_depth = jax.random.split(key)
    stride = MIX_TOKENS // 3
    places = jnp.arange(3, dtype=jnp.int32) * stride + jax.random.randint(key_place, (3,), 0, stride)
    kept = jax.random.uniform(key_depth, (3, HEADS), jnp.float32, 0.5, 0.8)
    positions = jnp.arange(MIX_TOKENS, dtype=jnp.int32)
    hits = (positions[None, :] == places[:, None]).astype(jnp.float32)
    return jnp.einsum('bh,bt->ht', jnp.log(kept), hits)


def draw_head_decay_logs(key, part):
    key_kind, key_fast, key_slow = jax.random.split(key, 3)
    fast_share = 0.5
    is_fast = jax.random.uniform(key_kind, (HEADS,), jnp.float32) < fast_share
    fast_log = jax.random.uniform(key_fast, (HEADS,), jnp.float32, math.log(1.0 / 40.0), math.log(1.0 / 15.0))
    slow_log = jax.random.uniform(key_slow, (HEADS,), jnp.float32, math.log(0.02), math.log(0.25)) - math.log(float(MIX_TOKENS))
    return jnp.where(is_fast, fast_log, slow_log)


def shard_levels(key, shape, cuts, smallest, high):
    loudness, own = 1.0, jax.random.fold_in(key, 6)
    for position, blocks in cuts:
        draws = jnp.exp(jax.random.uniform(jax.random.fold_in(own, position), (blocks,), jnp.float32, smallest / len(cuts), high / len(cuts)))
        loudness = loudness * jnp.repeat(draws, shape[position] // blocks).reshape([-1 if axis == position else 1 for axis in range(len(shape))])
    return loudness


def deal_out(key, own, number, rows, amount, top, limit, skew):
    sequence = jax.random.permutation(key, amount)
    packed, ordinary = load_shares(amount, rows * top, limit, skew, True), load_shares(amount, rows * top, limit, skew, False)
    places = jnp.arange(amount)

    def named(tallies, rotation):
        used = int((tallies > 0).sum())
        fixed = max(1, used // 4)
        passed = fixed + (places - fixed + rotation * (used - fixed)) % max(1, amount - fixed)
        return jnp.zeros((amount,), jnp.int32).at[sequence[jnp.where(places < fixed, places, passed)]].set(jnp.asarray(tallies, jnp.int32))

    tallies = jnp.where(number % 4 == 0, named(packed, number // 4), named(ordinary, number - number // 4 - 1))
    mixed = jax.random.permutation(jax.random.fold_in(own, 3), amount)
    giver, taker = mixed[0:amount // 2 * 2:2], mixed[1:amount // 2 * 2:2]
    margin = jnp.minimum(tallies[giver] - 1, limit - tallies[taker]) // 2
    margin = jnp.where((giver == sequence[0]) | (taker == sequence[0]) | (tallies[taker] == 0), 0, jnp.maximum(margin, 0))
    passed = jax.random.randint(jax.random.fold_in(own, 4), (amount // 2,), 0, 1 << 20) % (margin + 1)
    tallies = tallies.at[giver].add(-passed).at[taker].add(passed)
    items = jnp.searchsorted(jnp.cumsum(tallies), jnp.arange(rows * top), side="right").astype(jnp.int32)
    grid = items.reshape(top, rows).T
    grid = grid[jax.random.permutation(jax.random.fold_in(own, 1), rows)]
    rotation = jax.random.randint(jax.random.fold_in(own, 2), (rows, 1), 0, top)
    return jnp.take_along_axis(grid, (jnp.arange(top)[None, :] + rotation) % top, axis=1)


def load_shares(number_of, total, most, lean, full):
    weights = [(1 << 20) // math.isqrt(grade ** lean) + 1 for grade in range(1, number_of + 1)]
    largest = most if full else min(most, max(-(-total // number_of), total * weights[0] // sum(weights)))
    least = 1 if total - largest >= number_of - 1 else 0
    counts, surplus = [largest] + [least] * (number_of - 1), total - largest - least * (number_of - 1)
    while surplus > 0:
        candidates = [i for i in range(1, number_of) if counts[i] < largest] or [i for i in range(1, number_of) if counts[i] < most]
        whole, remaining = sum([weights[i] for i in candidates]), surplus
        for i in candidates:
            more = min(most - counts[i], max(1, remaining * weights[i] // whole), surplus)
            counts[i] = counts[i] + more
            surplus = surplus - more
    return np.array(counts)


def scatter_about(key, dims, deviation, bound, pieces=(), kind=jnp.bfloat16):
    level = shard_levels(key, dims, pieces, -0.22, 0.18) if pieces else 1.0
    result = jax.random.normal(key, dims, jnp.float32) * deviation * level
    return jnp.minimum(jnp.maximum(result, -bound), bound).astype(kind)


def setup_inputs(seed: int = 0) -> dict:
    streams_of = jax.random.split(jax.random.key(seed), 23)
    head_inputs_unfiltered = scatter_about(streams_of[0], (MIX_TOKENS, INNER), 1.0, 6.0, ((0, 64), (1, 4)))
    group_write_vectors = scatter_about(streams_of[1], (MIX_TOKENS, GROUPS * STATE), 1.0, 6.0, ((0, 64), (1, 4)))
    group_read_vectors = scatter_about(streams_of[2], (MIX_TOKENS, GROUPS * STATE), 1.0, 6.0, ((0, 64), (1, 4)))
    output_gate_inputs = scatter_about(streams_of[3], (MIX_TOKENS, INNER), 1.0, 6.0, ((0, 64), (1, 4)))
    step_preactivation = draw_step_preactivation(jax.random.fold_in(streams_of[22], 71), 0)
    extra_decay_logs = draw_extra_decay_logs(jax.random.fold_in(streams_of[22], 71), 0)
    head_decay_logs = draw_head_decay_logs(jax.random.fold_in(streams_of[22], 71), 0)
    head_filter_taps = scatter_about(streams_of[7], (CONV, INNER), 0.5, 3.0, ((1, 4),))
    write_filter_taps = scatter_about(streams_of[8], (CONV, GROUPS * STATE), 0.5, 3.0, ((1, 4),))
    read_filter_taps = scatter_about(streams_of[9], (CONV, GROUPS * STATE), 0.5, 3.0, ((1, 4),))
    grouped_norm_gain = jnp.clip(1.0 + 0.18 * jax.random.normal(streams_of[10], (INNER,), jnp.float32), 0.1, 1.9)
    mixer_output_weight = scatter_about(streams_of[11], (INNER, D), INNER ** -0.5, 0.09375, ((0, 4),))
    expert_input_rows = scatter_about(streams_of[12], (MOE_TOKENS, D), 1.0, 6.0, ((0, 256),))
    expert_norm_gain = jnp.clip(1.0 + 0.18 * jax.random.normal(streams_of[13], (D,), jnp.float32), 0.1, 1.9)
    routes_keys = jax.random.split(jax.random.fold_in(streams_of[14], 1), MOE_TOKENS // MOE_ROWS)
    routes_turns = jax.random.permutation(jax.random.fold_in(streams_of[14], 3), MOE_TOKENS // MOE_ROWS)
    routes = jax.vmap(lambda own, number: deal_out(jax.random.fold_in(streams_of[14], 2), own, number, MOE_ROWS, EXPERTS, TOP_K, CAPACITY, 2))(routes_keys, routes_turns).reshape((MOE_TOKENS, TOP_K))
    router_chosen_scores = jnp.clip(jnp.exp(math.log(1.0) - 2.9996462 * jax.random.uniform(streams_of[15], (MOE_TOKENS, TOP_K), jnp.float32) ** shard_levels(streams_of[15], (MOE_TOKENS, TOP_K), ((0, 256),), -0.2, 0.2)), 0.049804688, 1.0).astype(jnp.bfloat16)
    routed_gate_weight = scatter_about(streams_of[16], (EXPERTS, D, EXPERT_FF), D ** -0.5, 0.125, ((0, 64), (2, 4)))
    routed_up_weight = scatter_about(streams_of[17], (EXPERTS, D, EXPERT_FF), D ** -0.5, 0.125, ((0, 64), (2, 4)))
    routed_down_weight = scatter_about(streams_of[18], (EXPERTS, EXPERT_FF, D), EXPERT_FF ** -0.5, 0.1875, ((0, 64), (1, 4)))
    shared_gate_weight = scatter_about(streams_of[19], (D, SHARED_FF), D ** -0.5, 0.125, ((1, 4),))
    shared_up_weight = scatter_about(streams_of[20], (D, SHARED_FF), D ** -0.5, 0.125, ((1, 4),))
    shared_down_weight = scatter_about(streams_of[21], (SHARED_FF, D), SHARED_FF ** -0.5, 0.25, ((0, 4),))
    return dict(head_inputs_unfiltered=head_inputs_unfiltered, group_write_vectors=group_write_vectors, group_read_vectors=group_read_vectors, output_gate_inputs=output_gate_inputs, step_preactivation=step_preactivation, extra_decay_logs=extra_decay_logs, head_decay_logs=head_decay_logs, head_filter_taps=head_filter_taps, write_filter_taps=write_filter_taps, read_filter_taps=read_filter_taps, grouped_norm_gain=grouped_norm_gain, mixer_output_weight=mixer_output_weight, expert_input_rows=expert_input_rows, expert_norm_gain=expert_norm_gain, routes=routes, router_chosen_scores=router_chosen_scores, routed_gate_weight=routed_gate_weight, routed_up_weight=routed_up_weight, routed_down_weight=routed_down_weight, shared_gate_weight=shared_gate_weight, shared_up_weight=shared_up_weight, shared_down_weight=shared_down_weight)


eps_norm = 1e-06
route_scale = 2.5
highest = lax.Precision.HIGHEST

def causal_conv(values, weights):
    taps = weights.shape[0]
    length = values.shape[0]
    padded = jnp.concatenate([jnp.zeros((taps - 1, values.shape[1]), jnp.float32), values.astype(jnp.float32)], axis=0)
    running_sum = jnp.zeros((length, values.shape[1]), jnp.float32)
    for offset in range(taps):
        running_sum = running_sum + weights[offset].astype(jnp.float32) * padded[offset:offset + length]
    return jax.nn.silu(running_sum)

def state_space(head_values, write_values, read_values, step_length_value, decay_rate_logs):
    length = head_values.shape[0]
    block_count = length // BLOCK
    per_group = HEADS // GROUPS
    head_blocks = head_values.reshape(block_count, BLOCK, GROUPS, per_group, HEAD_DIM)
    write_blocks = write_values.reshape(block_count, BLOCK, GROUPS, STATE)
    read_blocks = read_values.reshape(block_count, BLOCK, GROUPS, STATE)
    step_blocks = step_length_value.T.reshape(block_count, BLOCK, GROUPS, per_group)
    rate_blocks = decay_rate_logs.T.reshape(block_count, BLOCK, GROUPS, per_group)
    lower_mask = jnp.tril(jnp.ones((BLOCK, BLOCK), bool))

    def advance(carried, block_data):
        head_blk, write_blk, read_blk, step_blk, rate_blk = block_data
        cumulative = jnp.cumsum(rate_blk, axis=0)
        weighted = head_blk * step_blk[..., None]
        gap_logs = cumulative[:, None] - cumulative[None, :]
        within = jnp.exp(jnp.where(lower_mask[:, :, None, None], gap_logs, -jnp.inf))
        affinity = jnp.einsum('lgn,sgn->lsg', read_blk, write_blk, precision=highest)
        local_part = jnp.einsum('lsge,sgep->lgep', affinity[..., None] * within, weighted, precision=highest)
        carried_part = jnp.einsum('lgn,gepn->lgep', read_blk, carried, precision=highest) * jnp.exp(cumulative)[..., None]
        to_end = jnp.exp(cumulative[-1:] - cumulative)
        new_state = carried * jnp.exp(cumulative[-1])[..., None, None] + jnp.einsum('sgn,sgep->gepn', write_blk, weighted * to_end[..., None], precision=highest)
        return (new_state, local_part + carried_part)
    initial = jnp.zeros((GROUPS, per_group, HEAD_DIM, STATE), jnp.float32)
    _, outputs = lax.scan(advance, initial, (head_blocks, write_blocks, read_blocks, step_blocks, rate_blocks))
    return outputs.reshape(length, HEADS * HEAD_DIM)

def reference(head_inputs_unfiltered, group_write_vectors, group_read_vectors, output_gate_inputs, step_preactivation, extra_decay_logs, head_decay_logs, head_filter_taps, write_filter_taps, read_filter_taps, grouped_norm_gain, mixer_output_weight, expert_input_rows, expert_norm_gain, routes, router_chosen_scores, routed_gate_weight, routed_up_weight, routed_down_weight, shared_gate_weight, shared_up_weight, shared_down_weight):
    length = head_inputs_unfiltered.shape[0]
    head_values = causal_conv(head_inputs_unfiltered, head_filter_taps)
    write_values = causal_conv(group_write_vectors, write_filter_taps)
    read_values = causal_conv(group_read_vectors, read_filter_taps)
    step_length_value = jax.nn.softplus(step_preactivation)
    decay_rate_logs = -jnp.exp(head_decay_logs)[:, None] * step_length_value + extra_decay_logs
    scan_out = state_space(head_values, write_values, read_values, step_length_value, decay_rate_logs)
    gated = scan_out * jax.nn.silu(output_gate_inputs.astype(jnp.float32))
    grouped = gated.reshape(length, GROUPS, HEADS * HEAD_DIM // GROUPS)
    grouped = grouped * lax.rsqrt(lax.optimization_barrier(jnp.mean(grouped * grouped, axis=-1, keepdims=True)) + eps_norm)
    mixer_normed = (grouped.reshape(length, HEADS * HEAD_DIM) * grouped_norm_gain).astype(jnp.bfloat16)
    mixer_result = jnp.dot(mixer_normed, mixer_output_weight, preferred_element_type=jnp.float32).astype(jnp.bfloat16)
    rows_float = expert_input_rows.astype(jnp.float32)
    moe_normed = (rows_float * lax.rsqrt(lax.optimization_barrier(jnp.mean(rows_float * rows_float, axis=-1, keepdims=True)) + eps_norm) * expert_norm_gain).astype(jnp.bfloat16)
    score_float = router_chosen_scores.astype(jnp.float32)
    route_weight = score_float / lax.optimization_barrier(jnp.sum(score_float, axis=-1, keepdims=True)) * route_scale
    token_total = expert_input_rows.shape[0]
    device_total = token_total // MOE_ROWS
    flat_expert = routes.reshape(device_total, MOE_ROWS * TOP_K)
    onehot = (flat_expert[:, :, None] == jnp.arange(EXPERTS, dtype=jnp.int32)[None, None, :]).astype(jnp.int32)
    before = jnp.cumsum(onehot, axis=1) - onehot
    slot_rank = lax.optimization_barrier(jnp.sum(before * onehot, axis=2))
    slot_index = jnp.arange(device_total, dtype=jnp.int32)[:, None] * CAPACITY + slot_rank
    token_index = jnp.arange(token_total * TOP_K, dtype=jnp.int32) // TOP_K
    table_token = jnp.full((EXPERTS, device_total * CAPACITY), token_total, jnp.int32).at[flat_expert.reshape(-1), slot_index.reshape(-1)].set(token_index)
    table_weight = jnp.zeros((EXPERTS, device_total * CAPACITY), jnp.float32).at[flat_expert.reshape(-1), slot_index.reshape(-1)].set(route_weight.reshape(-1))
    padded_rows = jnp.concatenate([moe_normed, jnp.zeros((1, D), jnp.bfloat16)], axis=0)
    slice_width = EXPERT_FF // N_TP

    def one_expert(running_sum, expert_data):
        tokens_here, weights_here, gate_weight, up_weight, down_weight = expert_data
        picked = padded_rows[tokens_here]
        gate_value = jnp.dot(picked, gate_weight, preferred_element_type=jnp.float32)
        up_value = jnp.dot(picked, up_weight, preferred_element_type=jnp.float32)
        hidden = (jax.nn.silu(gate_value) * up_value).astype(jnp.bfloat16)
        summed = jnp.zeros((picked.shape[0], D), jnp.float32)
        for slice_index in range(N_TP):
            lower_edge = slice_index * slice_width
            part = jnp.dot(hidden[:, lower_edge:lower_edge + slice_width], down_weight[lower_edge:lower_edge + slice_width], preferred_element_type=jnp.float32).astype(jnp.bfloat16)
            summed = summed + part.astype(jnp.float32)
        return (running_sum.at[tokens_here].add(summed * weights_here[:, None]), None)
    routed, _ = lax.scan(one_expert, jnp.zeros((token_total + 1, D), jnp.float32), (table_token, table_weight, routed_gate_weight, routed_up_weight, routed_down_weight))
    shared_hidden = (jax.nn.silu(jnp.dot(moe_normed, shared_gate_weight, preferred_element_type=jnp.float32)) * jnp.dot(moe_normed, shared_up_weight, preferred_element_type=jnp.float32)).astype(jnp.bfloat16)
    shared_total = jnp.dot(shared_hidden, shared_down_weight, preferred_element_type=jnp.float32)
    moe_result = (shared_total + routed[:token_total]).astype(jnp.bfloat16)
    return (mixer_result, moe_result)
```

```python
import functools

import jax
import jax.numpy as jnp
from jax import lax
from jax.experimental import pallas as pl
from jax.experimental.pallas import tpu as pltpu
from jax.sharding import Mesh
from jax.sharding import PartitionSpec as P


HEAD_DIM = 64
STATE = 128
LANE = 128
EP = ("ep_0", "ep_1", "ep_2")
EP_TP = ("ep_0", "ep_1", "ep_2", "tp")

eps_norm = 1e-06
route_scale = 2.5
highest = lax.Precision.HIGHEST
f32 = jnp.float32
bf16 = jnp.bfloat16


MIB = 1024 * 1024


def shift(value, axis, by, wrap):
    devices = lax.axis_size(axis)
    if wrap:
        pairs = [(i, (i + by) % devices) for i in range(devices)]
    else:
        pairs = [(i, i + by) for i in range(devices) if 0 <= i + by < devices]
    return lax.ppermute(value, axis, pairs)


def call(body, outs, scratch, mib):
    return pl.pallas_call(
        body,
        out_shape=outs,
        scratch_shapes=list(scratch),
        compiler_params=pltpu.CompilerParams(vmem_limit_bytes=mib * MIB),
    )


def dispatch_body(capacity, experts, x_ref, gain_ref, routes_ref, normed_ref, out_ref, scr):
    rows, width = x_ref.shape
    x = x_ref[...].astype(f32)
    scale = lax.rsqrt(jnp.mean(x * x, axis=-1, keepdims=True) + eps_norm)
    normed_ref[...] = (x * scale * gain_ref[...]).astype(bf16)
    first = routes_ref[0:1, :]
    second = routes_ref[1:2, :]
    names = lax.broadcasted_iota(jnp.int32, (experts, rows), 0)
    hit0 = (names == first).astype(f32)
    hit1 = (names == second).astype(f32)
    earlier = (
        lax.broadcasted_iota(jnp.int32, (rows, rows), 0)
        < lax.broadcasted_iota(jnp.int32, (rows, rows), 1)
    ).astype(bf16)
    before = jnp.dot((hit0 + hit1).astype(bf16), earlier, preferred_element_type=f32)
    slot0 = first * capacity + jnp.sum(before * hit0, axis=0, keepdims=True).astype(jnp.int32)
    slot1 = second * capacity + jnp.sum(before * hit1, axis=0, keepdims=True).astype(jnp.int32)
    slots = experts * capacity
    place = lax.broadcasted_iota(jnp.int32, (slots, rows), 0)
    pick = ((place == slot0) | (place == slot1)).astype(bf16)
    pieces = width // LANE
    for k in range(0, pieces, 2):
        part = jnp.dot(
            pick, normed_ref[:, k * LANE : (k + 2) * LANE], preferred_element_type=f32
        )
        scr[pl.ds(k, slots, stride=pieces), :] = part[:, :LANE]
        scr[pl.ds(k + 1, slots, stride=pieces), :] = part[:, LANE:]
    out_ref[...] = scr[...].astype(bf16)


def expert_hidden(x, gate, up):
    gate_value = jnp.dot(x, gate, preferred_element_type=f32)
    up_value = jnp.dot(x, up, preferred_element_type=f32)
    return (gate_value * jax.nn.sigmoid(gate_value) * up_value).astype(bf16)


def expert_first_body(in_ref, w0, w1, w2, rows_ref, sum_ref, scr):
    slots, width = rows_ref.shape
    pieces = width // LANE
    scr[...] = in_ref[...].astype(f32)
    for k in range(pieces):
        rows_ref[:, k * LANE : (k + 1) * LANE] = scr[pl.ds(k, slots, stride=pieces), :].astype(bf16)
    x = rows_ref[...]
    units = w0.shape[1]
    hidden = [expert_hidden(x, w[:width, :], w[width : 2 * width, :]) for w in (w0, w1, w2)]
    for j in range(width // units):
        rows = slice(2 * width + j * units, 2 * width + (j + 1) * units)
        sum_ref[:, j * units : (j + 1) * units] = (
            jnp.dot(hidden[0], w0[rows, :], preferred_element_type=f32)
            + jnp.dot(hidden[1], w1[rows, :], preferred_element_type=f32)
            + jnp.dot(hidden[2], w2[rows, :], preferred_element_type=f32)
        )


def expert_last_body(rows_ref, sum_ref, wa, wb, out_ref, scr):
    slots, width = rows_ref.shape
    pieces = width // LANE
    units = wa.shape[1]
    edge = wa.shape[0]
    x = rows_ref[...]
    gate_value = jnp.dot(x, wa[:width, :], preferred_element_type=f32)
    up_value = jnp.dot(x[:, : edge - width], wa[width:, :], preferred_element_type=f32) + jnp.dot(
        x[:, edge - width :], wb[: 2 * width - edge, :], preferred_element_type=f32
    )
    hidden = (gate_value * jax.nn.sigmoid(gate_value) * up_value).astype(bf16)
    for k in range(0, pieces, 2):
        row = 2 * width - edge + k // 2 * units
        part = sum_ref[:, k * LANE : (k + 2) * LANE] + jnp.dot(
            hidden, wb[row : row + units, :], preferred_element_type=f32
        )
        scr[pl.ds(k, slots, stride=pieces), :] = part[:, :LANE]
        scr[pl.ds(k + 1, slots, stride=pieces), :] = part[:, LANE:]
    out_ref[...] = scr[...].astype(bf16)


def shared_body(core_ref, n_ref, *refs):
    out_ref = refs[-1]
    held = refs[:-1]
    core = core_ref[0]
    half = n_ref.shape[1] // 2
    mine = n_ref[:, pl.ds(pl.multiple_of(core * half, LANE), half)]
    other = n_ref[:, pl.ds(pl.multiple_of((1 - core) * half, LANE), half)]
    count = len(held) // 2
    low = jnp.zeros((n_ref.shape[0], half), f32)
    high = jnp.zeros((n_ref.shape[0], half), f32)
    for q in range(count):
        a = held[q]
        b = held[count + q]
        gate_value = jnp.dot(mine, a[:half, :], preferred_element_type=f32) + jnp.dot(
            other, b[:half, :], preferred_element_type=f32
        )
        up_value = jnp.dot(mine, a[half : 2 * half, :], preferred_element_type=f32) + jnp.dot(
            other, b[half : 2 * half, :], preferred_element_type=f32
        )
        hidden = (gate_value * jax.nn.sigmoid(gate_value) * up_value).astype(bf16)
        blocks = half // LANE
        low += jnp.concatenate(
            [
                jnp.dot(
                    hidden,
                    a[2 * half + j * LANE : 2 * half + (j + 1) * LANE, :],
                    preferred_element_type=f32,
                )
                for j in range(blocks)
            ],
            axis=1,
        )
        high += jnp.concatenate(
            [
                jnp.dot(
                    hidden,
                    b[2 * half + j * LANE : 2 * half + (j + 1) * LANE, :],
                    preferred_element_type=f32,
                )
                for j in range(blocks)
            ],
            axis=1,
        )
    out_ref[:, pl.ds(pl.multiple_of(core * half, LANE), half)] = low
    out_ref[:, pl.ds(pl.multiple_of((1 - core) * half, LANE), half)] = high


def combine_body(capacity, experts, in_ref, routes_ref, scores_ref, shared_ref, out_ref, scr):
    rows, width = out_ref.shape
    pieces = width // LANE
    slots = experts * capacity
    scr[...] = in_ref[...].astype(f32)
    first = routes_ref[:, 0:1]
    second = routes_ref[:, 1:2]
    names = lax.broadcasted_iota(jnp.int32, (rows, experts), 1)
    hit0 = (names == first).astype(f32)
    hit1 = (names == second).astype(f32)
    earlier = (
        lax.broadcasted_iota(jnp.int32, (rows, rows), 1)
        < lax.broadcasted_iota(jnp.int32, (rows, rows), 0)
    ).astype(bf16)
    before = jnp.dot(earlier, (hit0 + hit1).astype(bf16), preferred_element_type=f32)
    slot0 = first * capacity + jnp.sum(before * hit0, axis=1, keepdims=True).astype(jnp.int32)
    slot1 = second * capacity + jnp.sum(before * hit1, axis=1, keepdims=True).astype(jnp.int32)
    place = lax.broadcasted_iota(jnp.int32, (rows, slots), 1)
    pick = jnp.concatenate(
        [(place == slot0).astype(bf16), (place == slot1).astype(bf16)], axis=0
    )
    scores = scores_ref[...].astype(f32)
    weights = scores / jnp.sum(scores, axis=1, keepdims=True) * route_scale
    w0 = weights[:, 0:1]
    w1 = weights[:, 1:2]
    for k in range(0, pieces, 2):
        both = jnp.concatenate(
            [
                scr[pl.ds(k, slots, stride=pieces), :].astype(bf16),
                scr[pl.ds(k + 1, slots, stride=pieces), :].astype(bf16),
            ],
            axis=1,
        )
        got = jnp.dot(pick, both, preferred_element_type=f32)
        cols = slice(k * LANE, (k + 2) * LANE)
        out_ref[:, cols] = (
            got[:rows] * w0 + got[rows:] * w1 + shared_ref[:, cols]
        ).astype(bf16)


def conv_silu(values, weights):
    taps = weights.shape[0]
    length = values.shape[0] - taps + 1
    running_sum = jnp.zeros((length, values.shape[1]), f32)
    for offset in range(taps):
        running_sum = running_sum + weights[offset].astype(f32) * values[
            offset : offset + length
        ].astype(f32)
    return jax.nn.silu(running_sum)


def mixer_rows(
    head_inputs_unfiltered,
    group_write_vectors,
    group_read_vectors,
    output_gate_inputs,
    step_preactivation,
    extra_decay_logs,
    head_decay_logs,
    head_filter_taps,
    write_filter_taps,
    read_filter_taps,
    grouped_norm_gain,
):
    row_total, head_chans = head_inputs_unfiltered.shape
    taps = head_filter_taps.shape[0]
    write_chans = group_write_vectors.shape[1]
    heads = step_preactivation.shape[0]
    groups = write_chans // STATE
    per_group = heads // groups
    ep_count = lax.axis_size(EP)
    step = jax.nn.softplus(step_preactivation)
    log_rate = -jnp.exp(head_decay_logs)[:, None] * step + extra_decay_logs
    upto = jnp.triu(jnp.ones((row_total, row_total), f32))
    cumulative = jnp.dot(log_rate, upto, precision=highest)
    device_decay = cumulative[:, -1]
    tail_rows = jnp.concatenate(
        [
            head_inputs_unfiltered[row_total - taps + 1 :],
            group_write_vectors[row_total - taps + 1 :],
            group_read_vectors[row_total - taps + 1 :],
        ],
        axis=1,
    )
    earlier = shift(tail_rows, EP, 1, False)
    padded_heads = jnp.concatenate([earlier[:, :head_chans], head_inputs_unfiltered], axis=0)
    padded_write = jnp.concatenate(
        [earlier[:, head_chans : head_chans + write_chans], group_write_vectors], axis=0
    )
    padded_read = jnp.concatenate(
        [earlier[:, head_chans + write_chans :], group_read_vectors], axis=0
    )
    head_values = conv_silu(padded_heads, head_filter_taps).reshape(
        row_total, groups, per_group, HEAD_DIM
    )
    write_values = conv_silu(padded_write, write_filter_taps).reshape(row_total, groups, STATE)
    read_values = conv_silu(padded_read, read_filter_taps).reshape(row_total, groups, STATE)
    cum = cumulative.reshape(groups, per_group, row_total)
    weighted = head_values * jnp.transpose(
        step.reshape(groups, per_group, row_total), (2, 0, 1)
    )[..., None]
    to_end = jnp.exp(cum[..., -1:] - cum)
    device_state = jnp.einsum(
        "sgn,sgep->gepn",
        write_values,
        weighted * jnp.transpose(to_end, (2, 0, 1))[..., None],
        precision=highest,
    )
    state_rows = heads * HEAD_DIM // ep_count
    split_decay = []
    rest = jnp.repeat(device_decay, ep_count // heads)
    for _ in range(3):
        piece = lax.reduce_precision(rest, 8, 7)
        split_decay.append(piece)
        rest = rest - piece
    decay_lanes = jnp.stack(split_decay, axis=1)
    decay_block = jnp.pad(decay_lanes[:, None, :], ((0, 0), (0, 15), (0, STATE - 3)))
    sent = jnp.concatenate(
        [
            device_state.reshape(ep_count, state_rows, STATE).astype(bf16),
            decay_block.astype(bf16),
        ],
        axis=1,
    )
    arrived = lax.all_to_all(sent, EP, 0, 0, tiled=True)
    held = arrived[:, :state_rows]
    decays = jnp.sum(arrived[:, state_rows, :3].astype(f32), axis=1)
    order = jnp.arange(ep_count)
    strictly = order[None, :] < order[:, None]
    ends = jnp.dot((order[None, :] <= order[:, None]).astype(f32), decays, precision=highest)
    carry = jnp.exp(
        jnp.where(strictly, (ends - decays)[:, None] - ends[None, :], -jnp.inf)
    )
    entering = jnp.dot(
        carry, held.reshape(ep_count, -1).astype(f32), precision=highest
    ).astype(bf16)
    returned = lax.all_to_all(entering.reshape(ep_count, state_rows, STATE), EP, 0, 0, tiled=True)
    incoming = returned.reshape(groups, per_group, HEAD_DIM, STATE).astype(f32)
    lower = jnp.tril(jnp.ones((row_total, row_total), bool))
    within = jnp.exp(jnp.where(lower, cum[..., :, None] - cum[..., None, :], -jnp.inf))
    affinity = jnp.einsum("lgn,sgn->gls", read_values, write_values, precision=highest)
    local_part = jnp.einsum(
        "gels,sgep->lgep", affinity[:, None] * within, weighted, precision=highest
    )
    carried_part = (
        jnp.einsum("lgn,gepn->lgep", read_values, incoming, precision=highest)
        * jnp.transpose(jnp.exp(cum), (2, 0, 1))[..., None]
    )
    scan_out = (local_part + carried_part).reshape(row_total, groups, per_group * HEAD_DIM)
    gate_values = jax.nn.silu(output_gate_inputs.astype(f32)).reshape(
        row_total, groups, per_group * HEAD_DIM
    )
    gated_rows = scan_out * gate_values
    gated_rows = gated_rows * lax.rsqrt(
        jnp.mean(gated_rows * gated_rows, axis=-1, keepdims=True) + eps_norm
    )
    return (gated_rows.reshape(row_total, head_chans) * grouped_norm_gain).astype(bf16)


def layer(
    head_inputs_unfiltered,
    group_write_vectors,
    group_read_vectors,
    output_gate_inputs,
    step_preactivation,
    extra_decay_logs,
    head_decay_logs,
    head_filter_taps,
    write_filter_taps,
    read_filter_taps,
    grouped_norm_gain,
    mixer_output_weight,
    expert_input_rows,
    expert_norm_gain,
    routes,
    router_chosen_scores,
    routed_gate_weight,
    routed_up_weight,
    routed_down_weight,
    shared_gate_weight,
    shared_up_weight,
    shared_down_weight,
):
    tp_count = lax.axis_size("tp")
    ep_count = lax.axis_size(EP)
    core = lax.axis_index("ep_2")
    rows, width = expert_input_rows.shape
    experts = routed_gate_weight.shape[0] * ep_count
    capacity = 3 * rows * routes.shape[1] // (2 * experts)
    slots = experts * capacity
    pieces = width // LANE

    units = routed_gate_weight.shape[2]
    own = jnp.concatenate(
        [
            routed_gate_weight[0],
            routed_up_weight[0],
            routed_down_weight[0]
            .reshape(units, width // units, units)
            .transpose(1, 0, 2)
            .reshape(width, units),
        ],
        axis=0,
    )
    from_low = shift(own, "tp", 1, True)
    from_high = shift(own, "tp", -1, True)

    normed, sent_rows = call(
        functools.partial(dispatch_body, capacity, experts),
        (
            jax.ShapeDtypeStruct((rows, width), bf16),
            jax.ShapeDtypeStruct((slots * pieces, LANE), bf16),
        ),
        [pltpu.VMEM((slots * pieces, LANE), f32)],
        16,
    )(expert_input_rows, expert_norm_gain[None, :], routes.T)
    arrived = lax.all_to_all(
        sent_rows.reshape(experts, capacity * pieces, LANE), EP, 0, 0, tiled=True
    ).reshape(slots * pieces, LANE)

    edge = own.shape[0] // 2
    far_a = shift(from_low[:edge], "tp", 1, True)
    far_b = shift(from_high[edge:], "tp", -1, True)

    mixer_normed = mixer_rows(
        head_inputs_unfiltered,
        group_write_vectors,
        group_read_vectors,
        output_gate_inputs,
        step_preactivation,
        extra_decay_logs,
        head_decay_logs,
        head_filter_taps,
        write_filter_taps,
        read_filter_taps,
        grouped_norm_gain,
    )
    mix_rows = mixer_normed.shape[0]
    mix_term = jnp.dot(mixer_normed, mixer_output_weight, preferred_element_type=f32).astype(bf16)
    tp_index = lax.axis_index("tp")
    block = mix_rows // tp_count
    mix_total = None
    for by in range(tp_count):
        target = (tp_index + by) % tp_count
        part = lax.dynamic_slice_in_dim(mix_term, target * block, block, 0)
        if by:
            part = shift(part, "tp", by, True)
        part = part.astype(f32)
        mix_total = part if mix_total is None else mix_total + part
    mixer_result = mix_total.astype(bf16)

    expert_rows, expert_sum = call(
        expert_first_body,
        (
            jax.ShapeDtypeStruct((slots, width), bf16),
            jax.ShapeDtypeStruct((slots, width), f32),
        ),
        [pltpu.VMEM((slots * pieces, LANE), f32)],
        32,
    )(arrived, own, from_low, from_high)
    sent_back = call(
        expert_last_body,
        jax.ShapeDtypeStruct((slots * pieces, LANE), bf16),
        [pltpu.VMEM((slots * pieces, LANE), f32)],
        24,
    )(expert_rows, expert_sum, far_a, far_b)
    returned = lax.all_to_all(
        sent_back.reshape(experts, capacity * pieces, LANE), EP, 0, 0, tiled=True
    ).reshape(slots * pieces, LANE)

    cut = width // 2
    shared_own = jnp.concatenate(
        [
            lax.dynamic_slice_in_dim(shared_gate_weight, core * cut, cut, 0),
            lax.dynamic_slice_in_dim(shared_up_weight, core * cut, cut, 0),
            lax.dynamic_slice_in_dim(shared_down_weight, core * cut, cut, 1)
            .reshape(LANE, cut // LANE, LANE)
            .transpose(1, 0, 2)
            .reshape(cut, LANE),
        ],
        axis=0,
    )
    shared_low = shift(shared_own, "tp", 1, True)
    shared_high = shift(shared_own, "tp", -1, True)
    middle = shared_own.shape[0] // 2
    shared_far = [
        shift(shared_low[:middle], "tp", 1, True),
        shift(shared_high[middle:], "tp", -1, True),
    ]
    shared_far = jnp.concatenate(shared_far, axis=0)
    shared_mine = [shared_own, shared_low, shared_high, shared_far]
    shared_other = [shift(w, "ep_2", 1, True) for w in shared_mine]
    shared_sum = pl.pallas_call(
        shared_body,
        out_shape=jax.ShapeDtypeStruct((rows, width), f32),
        in_specs=[pl.BlockSpec(memory_space=pltpu.SMEM)] + [pl.BlockSpec(memory_space=pltpu.VMEM)] * 9,
        compiler_params=pltpu.CompilerParams(vmem_limit_bytes=16 * MIB),
        name="shared",
    )(core[None].astype(jnp.int32), normed, *shared_mine, *shared_other)

    moe_result = call(
        functools.partial(combine_body, capacity, experts),
        jax.ShapeDtypeStruct((rows, width), bf16),
        [pltpu.VMEM((slots * pieces, LANE), f32)],
        16,
    )(returned, routes, router_chosen_scores, shared_sum)
    return (mixer_result, moe_result)


def solution(mesh):
    split = Mesh(mesh.devices.reshape(8, 4, 2, mesh.shape["tp"]), ("ep_0", "ep_1", "ep_2", "tp"))
    placed = (
        P(EP, "tp"),
        P(EP, "tp"),
        P(EP, "tp"),
        P(EP, "tp"),
        P("tp", EP),
        P("tp", EP),
        P("tp"),
        P(None, "tp"),
        P(None, "tp"),
        P(None, "tp"),
        P("tp"),
        P("tp", None),
        P(EP_TP, None),
        P(),
        P(EP_TP, None),
        P(EP_TP, None),
        P(EP, None, "tp"),
        P(EP, None, "tp"),
        P(EP, "tp", None),
        P(None, "tp"),
        P(None, "tp"),
        P("tp", None),
    )
    return jax.shard_map(
        layer,
        mesh=split,
        in_specs=placed,
        out_specs=(P(EP_TP, None), P(EP_TP, None)),
        check_vma=False,
    )
```

```python
import functools

import jax
import jax.numpy as jnp
from jax import lax
from jax.experimental import pallas as pl
from jax.experimental.pallas import tpu as pltpu
from jax.sharding import Mesh
from jax.sharding import PartitionSpec as P


HEAD_DIM = 64
STATE = 128
LANE = 128
EP = ("ep_0", "ep_1", "ep_2")
EP_TP = ("ep_0", "ep_1", "ep_2", "tp")

eps_norm = 1e-06
route_scale = 2.5
highest = lax.Precision.HIGHEST
f32 = jnp.float32
bf16 = jnp.bfloat16


MIB = 1024 * 1024


def shift(value, axis, by, wrap):
    devices = lax.axis_size(axis)
    if wrap:
        pairs = [(i, (i + by) % devices) for i in range(devices)]
    else:
        pairs = [(i, i + by) for i in range(devices) if 0 <= i + by < devices]
    return lax.ppermute(value, axis, pairs)


def call(body, outs, scratch, mib):
    return pl.pallas_call(
        body,
        out_shape=outs,
        scratch_shapes=list(scratch),
        compiler_params=pltpu.CompilerParams(vmem_limit_bytes=mib * MIB),
    )


def place_rows(capacity, experts, chunk_rows, x_ref, gain_ref, routes_ref, normed_ref, scr):
    rows, width = x_ref.shape
    x = x_ref[...].astype(f32)
    scale = lax.rsqrt(jnp.mean(x * x, axis=-1, keepdims=True) + eps_norm)
    normed_ref[...] = (x * scale * gain_ref[...]).astype(bf16)
    first = routes_ref[0:1, :]
    second = routes_ref[1:2, :]
    names = lax.broadcasted_iota(jnp.int32, (experts, rows), 0)
    hit0 = (names == first).astype(f32)
    hit1 = (names == second).astype(f32)
    earlier = (
        lax.broadcasted_iota(jnp.int32, (rows, rows), 0)
        < lax.broadcasted_iota(jnp.int32, (rows, rows), 1)
    ).astype(bf16)
    before = jnp.dot((hit0 + hit1).astype(bf16), earlier, preferred_element_type=f32)
    slot0 = first + experts * jnp.sum(before * hit0, axis=0, keepdims=True).astype(jnp.int32)
    slot1 = second + experts * jnp.sum(before * hit1, axis=0, keepdims=True).astype(jnp.int32)
    slots = experts * capacity
    place = lax.broadcasted_iota(jnp.int32, (slots, rows), 0)
    pick = ((place == slot0) | (place == slot1)).astype(bf16)
    pieces = width // LANE
    for k in range(0, pieces, 2):
        part = jnp.dot(
            pick, normed_ref[:, k * LANE : (k + 2) * LANE], preferred_element_type=f32
        )
        for r in range(capacity):
            own = part[r * experts : (r + 1) * experts, :]
            row = r * pieces + k
            scr[pl.ds(row, experts, stride=chunk_rows), :] = own[:, :LANE]
            scr[pl.ds(row + 1, experts, stride=chunk_rows), :] = own[:, LANE:]


def expert_hidden(x, gate, up):
    gate_value = jnp.dot(x, gate, preferred_element_type=f32)
    up_value = jnp.dot(x, up, preferred_element_type=f32)
    return (gate_value * jax.nn.sigmoid(gate_value) * up_value).astype(bf16)


def expert_first_body(
    capacity, chunk_rows, in_ref, g0, u0, d0, g1, u1, d1a, d1b, g2, u2, d2a, d2b, rows_ref, sum_ref, scr
):
    slots, width = rows_ref.shape
    pieces = width // LANE
    sources = slots // capacity
    scr[...] = in_ref[...].astype(f32)
    for r in range(capacity):
        for k in range(pieces):
            got = scr[pl.ds(r * pieces + k, sources, stride=chunk_rows), :]
            rows_ref[r * sources : (r + 1) * sources, k * LANE : (k + 1) * LANE] = got.astype(bf16)
    x = rows_ref[...]
    hidden = [expert_hidden(x, g[...], u[...]) for g, u in ((g0, u0), (g1, u1), (g2, u2))]
    half = d1a.shape[0]
    for k in range(0, pieces, 2):
        cols = slice(k * LANE, (k + 2) * LANE)
        sum_ref[:, cols] = (
            jnp.dot(hidden[0], d0[:, cols], preferred_element_type=f32)
            + jnp.dot(hidden[1][:, :half], d1a[:, cols], preferred_element_type=f32)
            + jnp.dot(hidden[1][:, half:], d1b[:, cols], preferred_element_type=f32)
            + jnp.dot(hidden[2][:, :half], d2a[:, cols], preferred_element_type=f32)
            + jnp.dot(hidden[2][:, half:], d2b[:, cols], preferred_element_type=f32)
        )


def expert_hidden_body(rows_ref, g, u, hidden_ref):
    hidden_ref[...] = expert_hidden(rows_ref[...], g[...], u[...])


def expert_last_body(capacity, hidden_ref, sum_ref, da, db, out_ref, scr):
    slots, width = sum_ref.shape
    pieces = width // LANE
    hidden = hidden_ref[...]
    half = da.shape[0]
    for k in range(0, pieces, 2):
        cols = slice(k * LANE, (k + 2) * LANE)
        part = (
            sum_ref[:, cols]
            + jnp.dot(hidden[:, :half], da[:, cols], preferred_element_type=f32)
            + jnp.dot(hidden[:, half:], db[:, cols], preferred_element_type=f32)
        )
        sources = slots // capacity
        for r in range(capacity):
            own = part[r * sources : (r + 1) * sources, :]
            row = r * pieces + k
            scr[pl.ds(row, sources, stride=capacity * pieces), :] = own[:, :LANE]
            scr[pl.ds(row + 1, sources, stride=capacity * pieces), :] = own[:, LANE:]
    out_ref[...] = scr[...].astype(bf16)


def shared_pack_body(core_ref, gate_ref, up_ref, down_ref, out_ref):
    width, chans = gate_ref.shape
    half = chans // 2
    core = core_ref[0]
    gate = gate_ref[...].astype(f32)
    up = up_ref[...].astype(f32)
    left = lax.broadcasted_iota(jnp.int32, (width, chans), 1) < half
    first = jnp.where(left, gate, pltpu.roll(up, half, 1))
    second = jnp.where(left, pltpu.roll(gate, half, 1), up)
    out_ref[:width, :] = jnp.where(core == 0, first, second).astype(bf16)
    rows = pl.multiple_of(core * half, half)
    for j in range(width // LANE):
        out_ref[width + j * half : width + (j + 1) * half, :] = down_ref[
            pl.ds(rows, half), j * LANE : (j + 1) * LANE
        ]


def shared_body(mine_ref, other_ref, own, low, high, far, sum_ref, send_ref):
    rows, width = mine_ref.shape
    x = jnp.concatenate([mine_ref[...], other_ref[...]], axis=0)
    lanes = lax.broadcasted_iota(jnp.int32, (2 * rows, LANE), 1) < LANE // 2
    packs = (own, low, high, far)
    hidden = []
    for pair in (packs[:2], packs[2:]):
        halves = []
        for pack in pair:
            both = jnp.dot(x, pack[:width, :], preferred_element_type=f32)
            up_value = pltpu.roll(both, LANE // 2, 1)
            halves.append(both * jax.nn.sigmoid(both) * up_value)
        hidden.append(jnp.where(lanes, halves[0], pltpu.roll(halves[1], LANE // 2, 1)))
    hidden = jnp.concatenate(hidden, axis=1).astype(bf16)
    units = LANE // 2
    for j in range(0, width // LANE, 2):
        down = jnp.concatenate(
            [
                jnp.concatenate(
                    [pack[width + i * units : width + (i + 1) * units, :] for pack in packs], axis=0
                )
                for i in (j, j + 1)
            ],
            axis=1,
        )
        part = jnp.dot(hidden, down, preferred_element_type=f32)
        cols = slice(j * LANE, (j + 2) * LANE)
        sum_ref[:, cols] = part[:rows]
        send_ref[:, cols] = part[rows:].astype(bf16)


def combine_body(
    capacity, experts, in_ref, routes_ref, scores_ref, shared_ref, other_ref, out_ref, scr
):
    rows, width = out_ref.shape
    pieces = width // LANE
    slots = experts * capacity
    scr[...] = in_ref[...].astype(f32)
    first = routes_ref[:, 0:1]
    second = routes_ref[:, 1:2]
    names = lax.broadcasted_iota(jnp.int32, (rows, experts), 1)
    hit0 = (names == first).astype(f32)
    hit1 = (names == second).astype(f32)
    earlier = (
        lax.broadcasted_iota(jnp.int32, (rows, rows), 1)
        < lax.broadcasted_iota(jnp.int32, (rows, rows), 0)
    ).astype(bf16)
    before = jnp.dot(earlier, (hit0 + hit1).astype(bf16), preferred_element_type=f32)
    slot0 = first * capacity + jnp.sum(before * hit0, axis=1, keepdims=True).astype(jnp.int32)
    slot1 = second * capacity + jnp.sum(before * hit1, axis=1, keepdims=True).astype(jnp.int32)
    place = lax.broadcasted_iota(jnp.int32, (rows, slots), 1)
    pick = jnp.concatenate(
        [(place == slot0).astype(bf16), (place == slot1).astype(bf16)], axis=0
    )
    scores = scores_ref[...].astype(f32)
    weights = scores / jnp.sum(scores, axis=1, keepdims=True) * route_scale
    w0 = weights[:, 0:1]
    w1 = weights[:, 1:2]
    for k in range(0, pieces, 2):
        both = jnp.concatenate(
            [
                scr[pl.ds(k, slots, stride=pieces), :].astype(bf16),
                scr[pl.ds(k + 1, slots, stride=pieces), :].astype(bf16),
            ],
            axis=1,
        )
        got = jnp.dot(pick, both, preferred_element_type=f32)
        cols = slice(k * LANE, (k + 2) * LANE)
        out_ref[:, cols] = (
            got[:rows] * w0
            + got[rows:] * w1
            + (shared_ref[:, cols] + other_ref[:, cols].astype(f32))
        ).astype(bf16)


def conv_silu(x_ref, tail, taps_ref, pad_ref):
    rows, chans = x_ref.shape
    taps = taps_ref.shape[0]
    start = 8 - taps + 1
    pad_ref[8 : 8 + rows, :chans] = x_ref[...].astype(f32)
    pad_ref[start:8, :chans] = tail.astype(f32)
    weights = taps_ref[...].astype(f32)
    total = weights[0:1, :] * pad_ref[start : start + rows, :chans]
    for j in range(1, taps):
        total = total + weights[j : j + 1, :] * pad_ref[start + j : start + j + rows, :chans]
    return total * jax.nn.sigmoid(total)


def precise(a, b, contract=(1, 0)):
    return lax.dot_general(
        a,
        b,
        (((contract[0],), (contract[1],)), ((), ())),
        precision=highest,
        preferred_element_type=f32,
    )


def spread(heads, chans):
    head = lax.broadcasted_iota(jnp.int32, (heads, chans), 0)
    chan = lax.broadcasted_iota(jnp.int32, (heads, chans), 1)
    return (chan // (chans // heads) == head).astype(f32)


def front_body(capacity, experts, chunk_rows, *refs):
    inputs, refs = refs[:13], refs[13:]
    outputs, refs = refs[:5], refs[5:]
    held_in, refs = refs[:13], refs[13:]
    held_out, refs = refs[:5], refs[5:]
    scr, pad_ref, values_ref, in_sems, out_sems = refs
    arriving = [
        pltpu.make_async_copy(source, target, in_sems.at[i])
        for i, (source, target) in enumerate(zip(inputs, held_in))
    ]
    leaving = [
        pltpu.make_async_copy(source, target, out_sems.at[i])
        for i, (source, target) in enumerate(zip(held_out, outputs))
    ]
    for copy in arriving:
        copy.start()
    x_ref, gain_ref, routes_ref, heads_ref, write_ref, read_ref, tail_ref = held_in[:7]
    pre_ref, extra_ref, rate_ref, head_taps, write_taps, read_taps = held_in[7:]
    normed_ref, out_ref, local_ref, read_out, grow_out = held_out
    for copy in arriving[:3]:
        copy.wait()
    place_rows(capacity, experts, chunk_rows, x_ref, gain_ref, routes_ref, normed_ref, scr)
    leaving[0].start()
    for copy in arriving[3:]:
        copy.wait()
    rows, chans = heads_ref.shape
    heads = pre_ref.shape[0]
    tail = tail_ref[...]
    values_ref[...] = conv_silu(heads_ref, tail[:, :chans], head_taps, pad_ref)
    write = conv_silu(write_ref, tail[:, chans : chans + STATE], write_taps, pad_ref)
    read = conv_silu(read_ref, tail[:, chans + STATE :], read_taps, pad_ref)
    read_out[...] = read
    pre = pre_ref[...]
    step = jnp.maximum(pre, 0.0) + jnp.log1p(jnp.exp(-jnp.abs(pre)))
    heads_across = lax.broadcasted_iota(jnp.int32, (heads, heads), 1)
    heads_down = lax.broadcasted_iota(jnp.int32, (heads, heads), 0)
    rate = jnp.sum(
        jnp.where(heads_across == heads_down, jnp.exp(rate_ref[...]), 0.0), axis=1, keepdims=True
    )
    log_rate = -rate * step + extra_ref[...]
    row = lax.broadcasted_iota(jnp.int32, (rows, rows), 0)
    col = lax.broadcasted_iota(jnp.int32, (rows, rows), 1)
    lower = row >= col
    cum = precise(log_rate, (row <= col).astype(f32))
    cum_down = precise(lower.astype(f32), log_rate, (1, 1))
    step_down = precise((row == col).astype(f32), step, (1, 1))
    grow_out[...] = jnp.exp(cum_down)
    wide = spread(heads, chans)
    to_end = step_down * jnp.exp(cum_down[rows - 1 : rows, :] - cum_down)
    ending = values_ref[...] * precise(to_end, wide)
    state = precise(ending, write, (0, 0))
    chunks = experts
    base = chunk_rows - 24
    repeat = chunks // heads
    chunk = lax.broadcasted_iota(jnp.int32, (chunks, heads), 0)
    head = lax.broadcasted_iota(jnp.int32, (chunks, heads), 1)
    total = precise((chunk // repeat == head).astype(f32), cum)[:, rows - 1 : rows]
    top = total.astype(bf16).astype(f32)
    middle = (total - top).astype(bf16).astype(f32)
    bottom = total - top - middle
    lane = lax.broadcasted_iota(jnp.int32, (chunks, STATE), 1)
    decays = jnp.where(
        lane == 0, top, jnp.where(lane == 1, middle, jnp.where(lane == 2, bottom, 0.0))
    )
    for j in range(chunks):
        row = chunk_rows * j + base
        scr[row : row + 16, :] = state[16 * j : 16 * j + 16, :]
        scr[row + 16 : row + 24, :] = jnp.broadcast_to(decays[j : j + 1, :], (8, STATE))
    out_ref[...] = scr[...].astype(bf16)
    leaving[1].start()
    affinity = precise(read, write, (1, 1))
    left = lax.broadcasted_iota(jnp.int32, (rows, LANE), 1) < HEAD_DIM
    for pair in range(heads // 2):
        mixed = []
        for e in (2 * pair, 2 * pair + 1):
            gap = cum_down[:, e : e + 1] - cum[e : e + 1, :]
            within = jnp.exp(jnp.where(lower, gap, -jnp.inf))
            mixed.append(affinity * within * step[e : e + 1, :])
        cols = slice(pair * LANE, (pair + 1) * LANE)
        part = precise(jnp.concatenate(mixed, axis=0), values_ref[:, cols])
        local_ref[:, cols] = jnp.where(left, part[:rows], part[rows:])
    for copy in leaving[2:]:
        copy.start()
    for copy in leaving:
        copy.wait()


def carry_body(in_ref, out_ref, scr, sums):
    chunks = in_ref.shape[0]
    scr[...] = in_ref[...].astype(f32).reshape(scr.shape)
    lane = lax.broadcasted_iota(jnp.int32, (chunks, STATE), 1)
    pieces = scr[pl.ds(16, chunks, stride=24), :]
    decay = jnp.sum(jnp.where(lane < 3, pieces, 0.0), axis=1, keepdims=True)
    row = lax.broadcasted_iota(jnp.int32, (chunks, chunks), 0)
    col = lax.broadcasted_iota(jnp.int32, (chunks, chunks), 1)
    held = jnp.broadcast_to(decay, (chunks, STATE))
    ends = precise((row >= col).astype(f32), held)[:, :chunks]
    ends_across = precise(held, (row <= col).astype(f32), (0, 0))[0:1, :]
    carry = jnp.exp(jnp.where(row > col, ends - decay - ends_across, -jnp.inf))
    for r in range(0, 16, 2):
        both = jnp.concatenate(
            [
                scr[pl.ds(r, chunks, stride=24), :],
                scr[pl.ds(r + 1, chunks, stride=24), :],
            ],
            axis=1,
        )
        part = precise(carry, both)
        sums[pl.ds(r, chunks, stride=16), :] = part[:, :STATE]
        sums[pl.ds(r + 1, chunks, stride=16), :] = part[:, STATE:]
    out_ref[...] = sums[...].astype(bf16)


def mixer_out_body(
    place_ref, state_ref, read_ref, grow_ref, local_ref, gate_ref, gain_ref, weight_ref, *refs
):
    outs = refs[:-2]
    normed_ref, total_ref = refs[-2:]
    rows, chans = local_ref.shape
    heads = grow_ref.shape[1]
    carried = precise(read_ref[...], state_ref[...].astype(f32), (1, 1))
    scan_out = local_ref[...] + carried * precise(grow_ref[...], spread(heads, chans))
    gate = gate_ref[...].astype(f32)
    gated = scan_out * (gate * jax.nn.sigmoid(gate))
    gated = gated * lax.rsqrt(jnp.mean(gated * gated, axis=-1, keepdims=True) + eps_norm)
    normed_ref[...] = (gated * gain_ref[...]).astype(bf16)
    total_ref[...] = jnp.dot(normed_ref[...], weight_ref[...], preferred_element_type=f32)
    parts = len(outs)
    block = rows // parts
    for by, out in enumerate(outs):
        target = lax.rem(place_ref[0] + by, parts)
        out[...] = total_ref[pl.ds(pl.multiple_of(target * block, block), block), :].astype(bf16)


def layer(
    head_inputs_unfiltered,
    group_write_vectors,
    group_read_vectors,
    output_gate_inputs,
    step_preactivation,
    extra_decay_logs,
    head_decay_logs,
    head_filter_taps,
    write_filter_taps,
    read_filter_taps,
    grouped_norm_gain,
    mixer_output_weight,
    expert_input_rows,
    expert_norm_gain,
    routes,
    router_chosen_scores,
    routed_gate_weight,
    routed_up_weight,
    routed_down_weight,
    shared_gate_weight,
    shared_up_weight,
    shared_down_weight,
):
    tp_count = lax.axis_size("tp")
    tp_index = lax.axis_index("tp")
    ep_count = lax.axis_size(EP)
    core = lax.axis_index("ep_2")
    rows, width = expert_input_rows.shape
    experts = routed_gate_weight.shape[0] * ep_count
    capacity = 3 * rows * routes.shape[1] // (2 * experts)
    slots = experts * capacity
    pieces = width // LANE
    exchanged = (experts, capacity * pieces, LANE)

    mix_rows, head_chans = head_inputs_unfiltered.shape
    taps = head_filter_taps.shape[0]
    tail_rows = jnp.concatenate(
        [
            head_inputs_unfiltered[mix_rows - taps + 1 :],
            group_write_vectors[mix_rows - taps + 1 :],
            group_read_vectors[mix_rows - taps + 1 :],
        ],
        axis=1,
    )
    tail_rows = shift(tail_rows, EP, 1, False)
    gate, up, down = routed_gate_weight[0], routed_up_weight[0], routed_down_weight[0]
    low_gate = shift(gate, "tp", 1, True)
    high_gate = shift(gate, "tp", -1, True)
    low_up = shift(up, "tp", 1, True)
    high_up = shift(up, "tp", -1, True)

    heads = step_preactivation.shape[0]
    chunk_rows = capacity * pieces + 24
    front_in = (
        expert_input_rows,
        expert_norm_gain[None, :],
        routes.T,
        head_inputs_unfiltered,
        group_write_vectors,
        group_read_vectors,
        tail_rows,
        step_preactivation,
        extra_decay_logs,
        head_decay_logs[None, :],
        head_filter_taps,
        write_filter_taps,
        read_filter_taps,
    )
    front_out = (
        jax.ShapeDtypeStruct((rows, width), bf16),
        jax.ShapeDtypeStruct((experts * chunk_rows, LANE), bf16),
        jax.ShapeDtypeStruct((mix_rows, head_chans), f32),
        jax.ShapeDtypeStruct((mix_rows, STATE), f32),
        jax.ShapeDtypeStruct((mix_rows, heads), f32),
    )
    in_hbm = pl.BlockSpec(memory_space=pltpu.HBM)
    normed, sent, local_part, read_values, growth = pl.pallas_call(
        functools.partial(front_body, capacity, experts, chunk_rows),
        out_shape=front_out,
        in_specs=[in_hbm] * len(front_in),
        out_specs=(in_hbm,) * len(front_out),
        scratch_shapes=[pltpu.VMEM(v.shape, v.dtype) for v in front_in + front_out]
        + [
            pltpu.VMEM((experts * chunk_rows, LANE), f32),
            pltpu.VMEM((mix_rows + 8, head_chans), f32),
            pltpu.VMEM((mix_rows, head_chans), f32),
            pltpu.SemaphoreType.DMA((len(front_in),)),
            pltpu.SemaphoreType.DMA((len(front_out),)),
        ],
        compiler_params=pltpu.CompilerParams(vmem_limit_bytes=60 * MIB),
        name="front",
    )(*front_in)
    arrived = lax.all_to_all(
        sent.reshape(experts, chunk_rows, LANE), EP, 0, 0, tiled=True
    )
    half = down.shape[0] // 2
    down_a, down_b = down[:half], down[half:]
    low_down_a = shift(down_a, "tp", 1, True)
    high_down_b = shift(down_b, "tp", -1, True)
    low_down_b = shift(down_b, "tp", 1, True)
    high_down_a = shift(down_a, "tp", -1, True)
    partner = shift(normed, "ep_2", 1, True)
    far_gate = shift(low_gate, "tp", 1, True)
    far_up = shift(high_up, "tp", -1, True)
    far_down_a = shift(low_down_a, "tp", 1, True)
    far_down_b = shift(high_down_b, "tp", -1, True)
    entering = pl.pallas_call(
        carry_body,
        out_shape=jax.ShapeDtypeStruct((ep_count * 16, STATE), bf16),
        grid=(1,),
        in_specs=[
            pl.BlockSpec((ep_count, 24, STATE), lambda i: (0, capacity * pieces // 24, 0))
        ],
        out_specs=pl.BlockSpec((ep_count * 16, STATE), lambda i: (0, 0)),
        scratch_shapes=[
            pltpu.VMEM((ep_count * 24, STATE), f32),
            pltpu.VMEM((ep_count * 16, STATE), f32),
        ],
        compiler_params=pltpu.CompilerParams(vmem_limit_bytes=8 * MIB),
        name="carry",
    )(arrived)
    entering = lax.all_to_all(entering.reshape(ep_count, 16, STATE), EP, 0, 0, tiled=True)

    expert_rows, expert_sum = call(
        functools.partial(expert_first_body, capacity, chunk_rows),
        (
            jax.ShapeDtypeStruct((slots, width), bf16),
            jax.ShapeDtypeStruct((slots, width), f32),
        ),
        [pltpu.VMEM((experts * chunk_rows, LANE), f32)],
        50,
    )(
        arrived.reshape(experts * chunk_rows, LANE),
        gate,
        up,
        down,
        low_gate,
        low_up,
        low_down_a,
        low_down_b,
        high_gate,
        high_up,
        high_down_a,
        high_down_b,
    )
    far_hidden = call(
        expert_hidden_body, jax.ShapeDtypeStruct((slots, down.shape[0]), bf16), (), 16
    )(expert_rows, far_gate, far_up)
    sent_back = call(
        functools.partial(expert_last_body, capacity),
        jax.ShapeDtypeStruct((slots * pieces, LANE), bf16),
        [pltpu.VMEM((slots * pieces, LANE), f32)],
        24,
    )(far_hidden, expert_sum, far_down_a, far_down_b)
    returned = lax.all_to_all(sent_back.reshape(exchanged), EP, 0, 0, tiled=True)

    block = mix_rows // tp_count
    mix_parts = pl.pallas_call(
        mixer_out_body,
        out_shape=[jax.ShapeDtypeStruct((block, width), bf16)] * tp_count,
        in_specs=[pl.BlockSpec(memory_space=pltpu.SMEM)]
        + [pl.BlockSpec(memory_space=pltpu.VMEM)] * 7,
        scratch_shapes=[
            pltpu.VMEM((mix_rows, head_chans), bf16),
            pltpu.VMEM((mix_rows, width), f32),
        ],
        compiler_params=pltpu.CompilerParams(vmem_limit_bytes=20 * MIB),
        name="mixer_out",
    )(
        tp_index[None].astype(jnp.int32),
        entering.reshape(ep_count * 16, STATE),
        read_values,
        growth,
        local_part,
        output_gate_inputs,
        grouped_norm_gain[None, :],
        mixer_output_weight,
    )
    mix_parts = [shift(part, "tp", by, True) if by else part for by, part in enumerate(mix_parts)]
    mixer_result = sum(part.astype(f32) for part in mix_parts).astype(bf16)

    units = shared_down_weight.shape[0] // 2
    shared_own = pl.pallas_call(
        shared_pack_body,
        out_shape=jax.ShapeDtypeStruct((width + pieces * units, LANE), bf16),
        in_specs=[pl.BlockSpec(memory_space=pltpu.SMEM)]
        + [pl.BlockSpec(memory_space=pltpu.VMEM)] * 3,
        compiler_params=pltpu.CompilerParams(vmem_limit_bytes=8 * MIB),
        name="shared_pack",
    )(
        core[None].astype(jnp.int32),
        shared_gate_weight,
        shared_up_weight,
        shared_down_weight,
    )
    shared_low = shift(shared_own, "tp", 1, True)
    shared_high = shift(shared_own, "tp", -1, True)
    shared_far = shift(shared_low, "tp", 1, True)
    shared_sum, shared_send = call(
        shared_body,
        (
            jax.ShapeDtypeStruct((rows, width), f32),
            jax.ShapeDtypeStruct((rows, width), bf16),
        ),
        (),
        16,
    )(normed, partner, shared_own, shared_low, shared_high, shared_far)
    shared_got = shift(shared_send, "ep_2", 1, True)

    moe_result = call(
        functools.partial(combine_body, capacity, experts),
        jax.ShapeDtypeStruct((rows, width), bf16),
        [pltpu.VMEM((slots * pieces, LANE), f32)],
        16,
    )(
        returned.reshape(slots * pieces, LANE),
        routes,
        router_chosen_scores,
        shared_sum,
        shared_got,
    )
    return (mixer_result, moe_result)


def solution(mesh):
    split = Mesh(mesh.devices.reshape(8, 4, 2, mesh.shape["tp"]), ("ep_0", "ep_1", "ep_2", "tp"))
    placed = (
        P(EP, "tp"),
        P(EP, "tp"),
        P(EP, "tp"),
        P(EP, "tp"),
        P("tp", EP),
        P("tp", EP),
        P("tp"),
        P(None, "tp"),
        P(None, "tp"),
        P(None, "tp"),
        P("tp"),
        P("tp", None),
        P(EP_TP, None),
        P(),
        P(EP_TP, None),
        P(EP_TP, None),
        P(EP, None, "tp"),
        P(EP, None, "tp"),
        P(EP, "tp", None),
        P(None, "tp"),
        P(None, "tp"),
        P("tp", None),
    )
    return jax.shard_map(
        layer,
        mesh=split,
        in_specs=placed,
        out_specs=(P(EP_TP, None), P(EP_TP, None)),
        check_vma=False,
    )
```

```python
import functools

import jax
import jax.numpy as jnp
from jax import lax
from jax.experimental import pallas as pl
from jax.experimental.pallas import tpu as pltpu
from jax.sharding import Mesh
from jax.sharding import PartitionSpec as P


HEAD_DIM = 64
STATE = 128
LANE = 128
EP = ("ep_0", "ep_1", "ep_2")
EP_TP = ("ep_0", "ep_1", "ep_2", "tp")

eps_norm = 1e-06
route_scale = 2.5
highest = lax.Precision.HIGHEST
f32 = jnp.float32
bf16 = jnp.bfloat16


MIB = 1024 * 1024


def shift(value, axis, by, wrap):
    devices = lax.axis_size(axis)
    if wrap:
        pairs = [(i, (i + by) % devices) for i in range(devices)]
    else:
        pairs = [(i, i + by) for i in range(devices) if 0 <= i + by < devices]
    return lax.ppermute(value, axis, pairs)


def call(body, outs, scratch, mib):
    return pl.pallas_call(
        body,
        out_shape=outs,
        scratch_shapes=list(scratch),
        compiler_params=pltpu.CompilerParams(vmem_limit_bytes=mib * MIB),
    )


def place_rows(capacity, experts, chunk_rows, x_ref, gain_ref, routes_ref, normed_ref, scr):
    rows, width = x_ref.shape
    x = x_ref[...].astype(f32)
    scale = lax.rsqrt(jnp.mean(x * x, axis=-1, keepdims=True) + eps_norm)
    normed_ref[...] = (x * scale * gain_ref[...]).astype(bf16)
    first = routes_ref[0:1, :]
    second = routes_ref[1:2, :]
    names = lax.broadcasted_iota(jnp.int32, (experts, rows), 0)
    hit0 = (names == first).astype(f32)
    hit1 = (names == second).astype(f32)
    earlier = (
        lax.broadcasted_iota(jnp.int32, (rows, rows), 0)
        < lax.broadcasted_iota(jnp.int32, (rows, rows), 1)
    ).astype(bf16)
    before = jnp.dot((hit0 + hit1).astype(bf16), earlier, preferred_element_type=f32)
    slot0 = first + experts * jnp.sum(before * hit0, axis=0, keepdims=True).astype(jnp.int32)
    slot1 = second + experts * jnp.sum(before * hit1, axis=0, keepdims=True).astype(jnp.int32)
    slots = experts * capacity
    place = lax.broadcasted_iota(jnp.int32, (slots, rows), 0)
    pick = ((place == slot0) | (place == slot1)).astype(bf16)
    pieces = width // LANE
    for k in range(0, pieces, 2):
        part = jnp.dot(
            pick, normed_ref[:, k * LANE : (k + 2) * LANE], preferred_element_type=f32
        )
        for r in range(capacity):
            own = part[r * experts : (r + 1) * experts, :]
            row = r * pieces + k
            scr[pl.ds(row, experts, stride=chunk_rows), :] = own[:, :LANE]
            scr[pl.ds(row + 1, experts, stride=chunk_rows), :] = own[:, LANE:]


def expert_hidden(x, gate, up):
    gate_value = jnp.dot(x, gate, preferred_element_type=f32)
    up_value = jnp.dot(x, up, preferred_element_type=f32)
    return (gate_value * jax.nn.sigmoid(gate_value) * up_value).astype(bf16)


def expert_first_body(
    capacity, chunk_rows, in_ref, g0, u0, g1, u1, g2, u2, d0, d1a, d1b, d2a, d2b, rows_ref, sum_ref, scr
):
    slots, width = rows_ref.shape
    pieces = width // LANE
    count = slots // capacity
    scr[...] = in_ref[...].astype(f32)
    for r in range(capacity):
        for k in range(pieces):
            got = scr[pl.ds(r * pieces + k, count, stride=chunk_rows), :]
            rows_ref[r * count : (r + 1) * count, k * LANE : (k + 1) * LANE] = got.astype(bf16)
    x = rows_ref[...]
    hidden = [expert_hidden(x, g[...], u[...]) for g, u in ((g0, u0), (g1, u1), (g2, u2))]
    for k in range(0, pieces, 2):
        cols = slice(k * LANE, (k + 2) * LANE)
        low_down = jnp.concatenate([d1a[:, cols], d1b[:, cols]], axis=0)
        high_down = jnp.concatenate([d2a[:, cols], d2b[:, cols]], axis=0)
        sum_ref[:, cols] = (
            jnp.dot(hidden[0], d0[:, cols], preferred_element_type=f32)
            + jnp.dot(hidden[1], low_down, preferred_element_type=f32)
            + jnp.dot(hidden[2], high_down, preferred_element_type=f32)
        )


def expert_hidden_body(rows_ref, g, u, hidden_ref):
    hidden_ref[...] = expert_hidden(rows_ref[...], g[...], u[...])


def expert_last_body(capacity, hidden_ref, sum_ref, da, db, out_ref, scr):
    slots, width = sum_ref.shape
    pieces = width // LANE
    hidden = hidden_ref[...]
    for k in range(0, pieces, 2):
        cols = slice(k * LANE, (k + 2) * LANE)
        part = (
            sum_ref[:, cols]
            + jnp.dot(
                hidden,
                jnp.concatenate([da[:, cols], db[:, cols]], axis=0),
                preferred_element_type=f32,
            )
        )
        sources = slots // capacity
        for r in range(capacity):
            own = part[r * sources : (r + 1) * sources, :]
            row = r * pieces + k
            scr[pl.ds(row, sources, stride=capacity * pieces), :] = own[:, :LANE]
            scr[pl.ds(row + 1, sources, stride=capacity * pieces), :] = own[:, LANE:]
    out_ref[...] = scr[...].astype(bf16)


def shared_pack_body(core_ref, gate_ref, up_ref, down_ref, out_ref):
    width, chans = gate_ref.shape
    half = chans // 2
    core = core_ref[0]
    gate = gate_ref[...].astype(f32)
    up = up_ref[...].astype(f32)
    left = lax.broadcasted_iota(jnp.int32, (width, chans), 1) < half
    first = jnp.where(left, gate, pltpu.roll(up, half, 1))
    second = jnp.where(left, pltpu.roll(gate, half, 1), up)
    out_ref[:width, :] = jnp.where(core == 0, first, second).astype(bf16)
    rows = pl.multiple_of(core * half, half)
    for j in range(width // LANE):
        out_ref[width + j * half : width + (j + 1) * half, :] = down_ref[
            pl.ds(rows, half), j * LANE : (j + 1) * LANE
        ]


def shared_body(mine_ref, other_ref, own, low, high, far, sum_ref, send_ref):
    rows, width = mine_ref.shape
    x = jnp.concatenate([mine_ref[...], other_ref[...]], axis=0)
    lanes = lax.broadcasted_iota(jnp.int32, (2 * rows, LANE), 1) < LANE // 2
    packs = (own, low, high, far)
    hidden = []
    for pair in (packs[:2], packs[2:]):
        halves = []
        for pack in pair:
            both = jnp.dot(x, pack[:width, :], preferred_element_type=f32)
            up_value = pltpu.roll(both, LANE // 2, 1)
            halves.append(both * jax.nn.sigmoid(both) * up_value)
        hidden.append(jnp.where(lanes, halves[0], pltpu.roll(halves[1], LANE // 2, 1)))
    hidden = jnp.concatenate(hidden, axis=1).astype(bf16)
    units = LANE // 2
    for j in range(0, width // LANE, 2):
        down = jnp.concatenate(
            [
                jnp.concatenate(
                    [pack[width + i * units : width + (i + 1) * units, :] for pack in packs], axis=0
                )
                for i in (j, j + 1)
            ],
            axis=1,
        )
        part = jnp.dot(hidden, down, preferred_element_type=f32)
        cols = slice(j * LANE, (j + 2) * LANE)
        sum_ref[:, cols] = part[:rows]
        send_ref[:, cols] = part[rows:].astype(bf16)


def combine_body(capacity, experts, in_ref, routes_ref, scores_ref, shared_ref, out_ref, scr):
    rows, width = out_ref.shape
    pieces = width // LANE
    slots = experts * capacity
    scr[...] = in_ref[...].astype(f32)
    first = routes_ref[:, 0:1]
    second = routes_ref[:, 1:2]
    names = lax.broadcasted_iota(jnp.int32, (rows, experts), 1)
    hit0 = (names == first).astype(f32)
    hit1 = (names == second).astype(f32)
    earlier = (
        lax.broadcasted_iota(jnp.int32, (rows, rows), 1)
        < lax.broadcasted_iota(jnp.int32, (rows, rows), 0)
    ).astype(bf16)
    before = jnp.dot(earlier, (hit0 + hit1).astype(bf16), preferred_element_type=f32)
    slot0 = first * capacity + jnp.sum(before * hit0, axis=1, keepdims=True).astype(jnp.int32)
    slot1 = second * capacity + jnp.sum(before * hit1, axis=1, keepdims=True).astype(jnp.int32)
    place = lax.broadcasted_iota(jnp.int32, (rows, slots), 1)
    pick = jnp.concatenate(
        [(place == slot0).astype(bf16), (place == slot1).astype(bf16)], axis=0
    )
    scores = scores_ref[...].astype(f32)
    weights = scores / jnp.sum(scores, axis=1, keepdims=True) * route_scale
    w0 = weights[:, 0:1]
    w1 = weights[:, 1:2]
    for k in range(0, pieces, 2):
        both = jnp.concatenate(
            [
                scr[pl.ds(k, slots, stride=pieces), :].astype(bf16),
                scr[pl.ds(k + 1, slots, stride=pieces), :].astype(bf16),
            ],
            axis=1,
        )
        got = jnp.dot(pick, both, preferred_element_type=f32)
        cols = slice(k * LANE, (k + 2) * LANE)
        out_ref[:, cols] = (
            got[:rows] * w0 + got[rows:] * w1 + shared_ref[:, cols]
        ).astype(bf16)


def conv_silu(x_ref, tail, taps_ref, pad_ref):
    rows, chans = x_ref.shape
    taps = taps_ref.shape[0]
    start = 8 - taps + 1
    pad_ref[8 : 8 + rows, :chans] = x_ref[...].astype(f32)
    pad_ref[start:8, :chans] = tail.astype(f32)
    weights = taps_ref[...].astype(f32)
    total = weights[0:1, :] * pad_ref[start : start + rows, :chans]
    for j in range(1, taps):
        total = total + weights[j : j + 1, :] * pad_ref[start + j : start + j + rows, :chans]
    return total * jax.nn.sigmoid(total)


def precise(a, b, contract=(1, 0)):
    return lax.dot_general(
        a,
        b,
        (((contract[0],), (contract[1],)), ((), ())),
        precision=highest,
        preferred_element_type=f32,
    )


def keep_near(value):
    return pltpu.with_memory_space_constraint(value, pltpu.VMEM)


def spread(heads, chans):
    head = lax.broadcasted_iota(jnp.int32, (heads, chans), 0)
    chan = lax.broadcasted_iota(jnp.int32, (heads, chans), 1)
    return (chan // (chans // heads) == head).astype(f32)


def front_body(capacity, experts, chunk_rows, *refs):
    inputs, refs = refs[:13], refs[13:]
    outputs, refs = refs[:5], refs[5:]
    held_in, refs = refs[:13], refs[13:]
    held_out, refs = refs[:5], refs[5:]
    scr, pad_ref, values_ref, in_sems, out_sems = refs
    arriving = [
        pltpu.make_async_copy(source, target, in_sems.at[i])
        for i, (source, target) in enumerate(zip(inputs, held_in))
    ]
    leaving = [
        pltpu.make_async_copy(source, target, out_sems.at[i])
        for i, (source, target) in enumerate(zip(held_out, outputs))
    ]
    for copy in arriving:
        copy.start()
    x_ref, gain_ref, routes_ref, heads_ref, write_ref, read_ref, tail_ref = held_in[:7]
    pre_ref, extra_ref, rate_ref, head_taps, write_taps, read_taps = held_in[7:]
    normed_ref, out_ref, local_ref, read_out, grow_out = held_out
    for copy in arriving[:3]:
        copy.wait()
    place_rows(capacity, experts, chunk_rows, x_ref, gain_ref, routes_ref, normed_ref, scr)
    leaving[0].start()
    for copy in arriving[3:]:
        copy.wait()
    rows, chans = heads_ref.shape
    heads = pre_ref.shape[0]
    tail = tail_ref[...]
    values_ref[...] = conv_silu(heads_ref, tail[:, :chans], head_taps, pad_ref)
    write = conv_silu(write_ref, tail[:, chans : chans + STATE], write_taps, pad_ref)
    read = conv_silu(read_ref, tail[:, chans + STATE :], read_taps, pad_ref)
    read_out[...] = read
    pre = pre_ref[...]
    step = jnp.maximum(pre, 0.0) + jnp.log1p(jnp.exp(-jnp.abs(pre)))
    heads_across = lax.broadcasted_iota(jnp.int32, (heads, heads), 1)
    heads_down = lax.broadcasted_iota(jnp.int32, (heads, heads), 0)
    rate = jnp.sum(
        jnp.where(heads_across == heads_down, jnp.exp(rate_ref[...]), 0.0), axis=1, keepdims=True
    )
    log_rate = -rate * step + extra_ref[...]
    row = lax.broadcasted_iota(jnp.int32, (rows, rows), 0)
    col = lax.broadcasted_iota(jnp.int32, (rows, rows), 1)
    lower = row >= col
    cum = precise(log_rate, (row <= col).astype(f32))
    cum_down = precise(lower.astype(f32), log_rate, (1, 1))
    step_down = precise((row == col).astype(f32), step, (1, 1))
    grow_out[...] = jnp.exp(cum_down)
    wide = spread(heads, chans)
    to_end = step_down * jnp.exp(cum_down[rows - 1 : rows, :] - cum_down)
    ending = values_ref[...] * precise(to_end, wide)
    state = precise(ending, write, (0, 0))
    chunks = experts
    base = chunk_rows - 24
    repeat = chunks // heads
    chunk = lax.broadcasted_iota(jnp.int32, (chunks, heads), 0)
    head = lax.broadcasted_iota(jnp.int32, (chunks, heads), 1)
    total = precise((chunk // repeat == head).astype(f32), cum)[:, rows - 1 : rows]
    top = total.astype(bf16).astype(f32)
    middle = (total - top).astype(bf16).astype(f32)
    bottom = total - top - middle
    lane = lax.broadcasted_iota(jnp.int32, (chunks, STATE), 1)
    decays = jnp.where(
        lane == 0, top, jnp.where(lane == 1, middle, jnp.where(lane == 2, bottom, 0.0))
    )
    for j in range(chunks):
        row = chunk_rows * j + base
        scr[row : row + 16, :] = state[16 * j : 16 * j + 16, :]
        scr[row + 16 : row + 24, :] = jnp.broadcast_to(decays[j : j + 1, :], (8, STATE))
    out_ref[...] = scr[...].astype(bf16)
    leaving[1].start()
    affinity = precise(read, write, (1, 1))
    left = lax.broadcasted_iota(jnp.int32, (rows, LANE), 1) < HEAD_DIM
    for pair in range(heads // 2):
        mixed = []
        for e in (2 * pair, 2 * pair + 1):
            gap = cum_down[:, e : e + 1] - cum[e : e + 1, :]
            within = jnp.exp(jnp.where(lower, gap, -jnp.inf))
            mixed.append(affinity * within * step[e : e + 1, :])
        cols = slice(pair * LANE, (pair + 1) * LANE)
        part = precise(jnp.concatenate(mixed, axis=0), values_ref[:, cols])
        local_ref[:, cols] = jnp.where(left, part[:rows], part[rows:])
    for copy in leaving[2:]:
        copy.start()
    for copy in leaving:
        copy.wait()


def carry_body(in_ref, out_ref, scr, sums):
    chunks = in_ref.shape[0]
    scr[...] = in_ref[...].astype(f32).reshape(scr.shape)
    lane = lax.broadcasted_iota(jnp.int32, (chunks, STATE), 1)
    pieces = scr[pl.ds(16, chunks, stride=24), :]
    decay = jnp.sum(jnp.where(lane < 3, pieces, 0.0), axis=1, keepdims=True)
    row = lax.broadcasted_iota(jnp.int32, (chunks, chunks), 0)
    col = lax.broadcasted_iota(jnp.int32, (chunks, chunks), 1)
    held = jnp.broadcast_to(decay, (chunks, STATE))
    ends = precise((row >= col).astype(f32), held)[:, :chunks]
    ends_across = precise(held, (row <= col).astype(f32), (0, 0))[0:1, :]
    carry = jnp.exp(jnp.where(row > col, ends - decay - ends_across, -jnp.inf))
    for r in range(0, 16, 2):
        both = jnp.concatenate(
            [
                scr[pl.ds(r, chunks, stride=24), :],
                scr[pl.ds(r + 1, chunks, stride=24), :],
            ],
            axis=1,
        )
        part = precise(carry, both)
        sums[pl.ds(r, chunks, stride=16), :] = part[:, :STATE]
        sums[pl.ds(r + 1, chunks, stride=16), :] = part[:, STATE:]
    out_ref[...] = sums[...].astype(bf16)


def mixer_out_body(
    place_ref, state_ref, read_ref, grow_ref, local_ref, gate_ref, gain_ref, weight_ref, *refs
):
    outs = refs[:-2]
    normed_ref, total_ref = refs[-2:]
    rows, chans = local_ref.shape
    heads = grow_ref.shape[1]
    carried = precise(read_ref[...], state_ref[...].astype(f32), (1, 1))
    scan_out = local_ref[...] + carried * precise(grow_ref[...], spread(heads, chans))
    gate = gate_ref[...].astype(f32)
    gated = scan_out * (gate * jax.nn.sigmoid(gate))
    gated = gated * lax.rsqrt(jnp.mean(gated * gated, axis=-1, keepdims=True) + eps_norm)
    normed_ref[...] = (gated * gain_ref[...]).astype(bf16)
    total_ref[...] = jnp.dot(normed_ref[...], weight_ref[...], preferred_element_type=f32)
    parts = len(outs)
    block = rows // parts
    for by, out in enumerate(outs):
        target = lax.rem(place_ref[0] + by, parts)
        out[...] = total_ref[pl.ds(pl.multiple_of(target * block, block), block), :].astype(bf16)


def layer(
    head_inputs_unfiltered,
    group_write_vectors,
    group_read_vectors,
    output_gate_inputs,
    step_preactivation,
    extra_decay_logs,
    head_decay_logs,
    head_filter_taps,
    write_filter_taps,
    read_filter_taps,
    grouped_norm_gain,
    mixer_output_weight,
    expert_input_rows,
    expert_norm_gain,
    routes,
    router_chosen_scores,
    routed_gate_weight,
    routed_up_weight,
    routed_down_weight,
    shared_gate_weight,
    shared_up_weight,
    shared_down_weight,
):
    tp_count = lax.axis_size("tp")
    tp_index = lax.axis_index("tp")
    ep_count = lax.axis_size(EP)
    core = lax.axis_index("ep_2")
    rows, width = expert_input_rows.shape
    experts = routed_gate_weight.shape[0] * ep_count
    capacity = 3 * rows * routes.shape[1] // (2 * experts)
    slots = experts * capacity
    pieces = width // LANE
    exchanged = (experts, capacity * pieces, LANE)

    mix_rows, head_chans = head_inputs_unfiltered.shape
    taps = head_filter_taps.shape[0]
    tail_rows = jnp.concatenate(
        [
            head_inputs_unfiltered[mix_rows - taps + 1 :],
            group_write_vectors[mix_rows - taps + 1 :],
            group_read_vectors[mix_rows - taps + 1 :],
        ],
        axis=1,
    )
    tail_rows = shift(tail_rows, EP, 1, False)
    gate, up, down = routed_gate_weight[0], routed_up_weight[0], routed_down_weight[0]
    low_gate = shift(gate, "tp", 1, True)
    high_gate = shift(gate, "tp", -1, True)
    low_up = shift(up, "tp", 1, True)
    high_up = shift(up, "tp", -1, True)

    heads = step_preactivation.shape[0]
    chunk_rows = capacity * pieces + 24
    front_in = (
        expert_input_rows,
        expert_norm_gain[None, :],
        routes.T,
        head_inputs_unfiltered,
        group_write_vectors,
        group_read_vectors,
        tail_rows,
        step_preactivation,
        extra_decay_logs,
        head_decay_logs[None, :],
        head_filter_taps,
        write_filter_taps,
        read_filter_taps,
    )
    front_out = (
        pltpu.HBM((rows, width), bf16),
        pltpu.HBM((experts * chunk_rows, LANE), bf16),
        pltpu.HBM((mix_rows, head_chans), f32),
        pltpu.HBM((mix_rows, STATE), f32),
        pltpu.HBM((mix_rows, heads), f32),
    )
    in_hbm = pl.BlockSpec(memory_space=pltpu.HBM)
    normed, sent, local_part, read_values, growth = pl.pallas_call(
        functools.partial(front_body, capacity, experts, chunk_rows),
        out_shape=front_out,
        in_specs=[in_hbm] * len(front_in),
        out_specs=(in_hbm,) * len(front_out),
        scratch_shapes=[pltpu.VMEM(v.shape, v.dtype) for v in front_in + front_out]
        + [
            pltpu.VMEM((experts * chunk_rows, LANE), f32),
            pltpu.VMEM((mix_rows + 8, head_chans), f32),
            pltpu.VMEM((mix_rows, head_chans), f32),
            pltpu.SemaphoreType.DMA((len(front_in),)),
            pltpu.SemaphoreType.DMA((len(front_out),)),
        ],
        compiler_params=pltpu.CompilerParams(vmem_limit_bytes=24 * MIB),
        name="front",
    )(*(pltpu.with_memory_space_constraint(v, pltpu.HBM) for v in front_in))
    arrived = lax.all_to_all(
        sent.reshape(experts, chunk_rows, LANE), EP, 0, 0, tiled=True
    )
    half = down.shape[0] // 2
    down_a, down_b = down[:half], down[half:]
    low_down_a = shift(down_a, "tp", 1, True)
    high_down_b = shift(down_b, "tp", -1, True)
    low_down_b = shift(down_b, "tp", 1, True)
    high_down_a = shift(down_a, "tp", -1, True)
    partner = shift(normed, "ep_2", 1, True)
    far_gate = shift(low_gate, "tp", 1, True)
    far_up = shift(high_up, "tp", -1, True)
    far_down_a = shift(low_down_a, "tp", 1, True)
    far_down_b = shift(high_down_b, "tp", -1, True)
    entering = pl.pallas_call(
        carry_body,
        out_shape=jax.ShapeDtypeStruct((ep_count * 16, STATE), bf16),
        grid=(1,),
        in_specs=[
            pl.BlockSpec((ep_count, 24, STATE), lambda i: (0, capacity * pieces // 24, 0))
        ],
        out_specs=pl.BlockSpec((ep_count * 16, STATE), lambda i: (0, 0)),
        scratch_shapes=[
            pltpu.VMEM((ep_count * 24, STATE), f32),
            pltpu.VMEM((ep_count * 16, STATE), f32),
        ],
        compiler_params=pltpu.CompilerParams(vmem_limit_bytes=8 * MIB),
        name="carry",
    )(arrived)
    entering = lax.all_to_all(entering.reshape(ep_count, 16, STATE), EP, 0, 0, tiled=True)

    low_gate, low_up, low_down_a, low_down_b = map(
        keep_near, (low_gate, low_up, low_down_a, low_down_b)
    )
    high_gate, high_up, high_down_a, high_down_b = map(
        keep_near, (high_gate, high_up, high_down_a, high_down_b)
    )
    far_gate, far_up, far_down_a, far_down_b = map(
        keep_near, (far_gate, far_up, far_down_a, far_down_b)
    )
    expert_rows, expert_sum = call(
        functools.partial(expert_first_body, capacity, chunk_rows),
        (pltpu.VMEM((slots, width), bf16), pltpu.VMEM((slots, width), f32)),
        [pltpu.VMEM((experts * chunk_rows, LANE), f32)],
        16,
    )(
        arrived.reshape(experts * chunk_rows, LANE),
        gate,
        up,
        low_gate,
        low_up,
        high_gate,
        high_up,
        down,
        low_down_a,
        low_down_b,
        high_down_a,
        high_down_b,
    )
    far_hidden = call(
        expert_hidden_body, jax.ShapeDtypeStruct((slots, down.shape[0]), bf16), (), 10
    )(expert_rows, far_gate, far_up)
    sent_back = call(
        functools.partial(expert_last_body, capacity),
        jax.ShapeDtypeStruct((slots * pieces, LANE), bf16),
        [pltpu.VMEM((slots * pieces, LANE), f32)],
        14,
    )(far_hidden, expert_sum, far_down_a, far_down_b)
    returned = lax.all_to_all(sent_back.reshape(exchanged), EP, 0, 0, tiled=True)

    block = mix_rows // tp_count
    mix_parts = pl.pallas_call(
        mixer_out_body,
        out_shape=[jax.ShapeDtypeStruct((block, width), bf16)] * tp_count,
        in_specs=[pl.BlockSpec(memory_space=pltpu.SMEM)]
        + [pl.BlockSpec(memory_space=pltpu.VMEM)] * 7,
        scratch_shapes=[
            pltpu.VMEM((mix_rows, head_chans), bf16),
            pltpu.VMEM((mix_rows, width), f32),
        ],
        compiler_params=pltpu.CompilerParams(vmem_limit_bytes=20 * MIB),
        name="mixer_out",
    )(
        tp_index[None].astype(jnp.int32),
        entering.reshape(ep_count * 16, STATE),
        read_values,
        growth,
        local_part,
        output_gate_inputs,
        grouped_norm_gain[None, :],
        mixer_output_weight,
    )
    mix_parts = [shift(part, "tp", by, True) if by else part for by, part in enumerate(mix_parts)]
    mixer_result = sum(part.astype(f32) for part in mix_parts).astype(bf16)

    units = shared_down_weight.shape[0] // 2
    shared_own = pl.pallas_call(
        shared_pack_body,
        out_shape=jax.ShapeDtypeStruct((width + pieces * units, LANE), bf16),
        in_specs=[pl.BlockSpec(memory_space=pltpu.SMEM)]
        + [pl.BlockSpec(memory_space=pltpu.VMEM)] * 3,
        compiler_params=pltpu.CompilerParams(vmem_limit_bytes=8 * MIB),
        name="shared_pack",
    )(
        core[None].astype(jnp.int32),
        shared_gate_weight,
        shared_up_weight,
        shared_down_weight,
    )
    shared_low = shift(shared_own, "tp", 1, True)
    shared_high = shift(shared_own, "tp", -1, True)
    shared_far = shift(shared_low, "tp", 1, True)
    shared_sum, shared_send = call(
        shared_body,
        (
            pltpu.HBM((rows, width), f32),
            jax.ShapeDtypeStruct((rows, width), bf16),
        ),
        (),
        16,
    )(normed, partner, shared_own, shared_low, shared_high, shared_far)
    shared_got = shift(shared_send, "ep_2", 1, True)

    moe_result = call(
        functools.partial(combine_body, capacity, experts),
        jax.ShapeDtypeStruct((rows, width), bf16),
        [pltpu.VMEM((slots * pieces, LANE), f32)],
        16,
    )(
        returned.reshape(slots * pieces, LANE),
        routes,
        router_chosen_scores,
        shared_sum + shared_got.astype(f32),
    )
    return (mixer_result, moe_result)


def solution(mesh):
    split = Mesh(mesh.devices.reshape(8, 4, 2, mesh.shape["tp"]), ("ep_0", "ep_1", "ep_2", "tp"))
    placed = (
        P(EP, "tp"),
        P(EP, "tp"),
        P(EP, "tp"),
        P(EP, "tp"),
        P("tp", EP),
        P("tp", EP),
        P("tp"),
        P(None, "tp"),
        P(None, "tp"),
        P(None, "tp"),
        P("tp"),
        P("tp", None),
        P(EP_TP, None),
        P(),
        P(EP_TP, None),
        P(EP_TP, None),
        P(EP, None, "tp"),
        P(EP, None, "tp"),
        P(EP, "tp", None),
        P(None, "tp"),
        P(None, "tp"),
        P("tp", None),
    )
    return jax.shard_map(
        layer,
        mesh=split,
        in_specs=placed,
        out_specs=(P(EP_TP, None), P(EP_TP, None)),
        check_vma=False,
    )
```

```python
import functools

import jax
import jax.numpy as jnp
from jax import lax
from jax.experimental import pallas as pl
from jax.experimental.pallas import tpu as pltpu
from jax.sharding import Mesh
from jax.sharding import PartitionSpec as P


HEAD_DIM = 64
STATE = 128
LANE = 128
EP = ("ep_0", "ep_1", "ep_2")
EP_TP = ("ep_0", "ep_1", "ep_2", "tp")

eps_norm = 1e-06
route_scale = 2.5
highest = lax.Precision.HIGHEST
f32 = jnp.float32
bf16 = jnp.bfloat16


MIB = 1024 * 1024


def shift(value, axis, by, wrap):
    devices = lax.axis_size(axis)
    if wrap:
        pairs = [(i, (i + by) % devices) for i in range(devices)]
    else:
        pairs = [(i, i + by) for i in range(devices) if 0 <= i + by < devices]
    return lax.ppermute(value, axis, pairs)


def call(body, outs, scratch, mib):
    return pl.pallas_call(
        body,
        out_shape=outs,
        scratch_shapes=list(scratch),
        compiler_params=pltpu.CompilerParams(vmem_limit_bytes=mib * MIB),
    )


def place_rows(capacity, experts, chunk_rows, x_ref, gain_ref, routes_ref, normed_ref, scr):
    rows, width = x_ref.shape
    x = x_ref[...].astype(f32)
    scale = lax.rsqrt(jnp.mean(x * x, axis=-1, keepdims=True) + eps_norm)
    normed_ref[...] = (x * scale * gain_ref[...]).astype(bf16)
    first = routes_ref[0:1, :]
    second = routes_ref[1:2, :]
    names = lax.broadcasted_iota(jnp.int32, (experts, rows), 0)
    hit0 = (names == first).astype(f32)
    hit1 = (names == second).astype(f32)
    earlier = (
        lax.broadcasted_iota(jnp.int32, (rows, rows), 0)
        < lax.broadcasted_iota(jnp.int32, (rows, rows), 1)
    ).astype(bf16)
    before = jnp.dot((hit0 + hit1).astype(bf16), earlier, preferred_element_type=f32)
    slot0 = first + experts * jnp.sum(before * hit0, axis=0, keepdims=True).astype(jnp.int32)
    slot1 = second + experts * jnp.sum(before * hit1, axis=0, keepdims=True).astype(jnp.int32)
    slots = experts * capacity
    place = lax.broadcasted_iota(jnp.int32, (slots, rows), 0)
    pick = ((place == slot0) | (place == slot1)).astype(bf16)
    pieces = width // LANE
    for k in range(0, pieces, 2):
        part = jnp.dot(
            pick, normed_ref[:, k * LANE : (k + 2) * LANE], preferred_element_type=f32
        )
        for r in range(capacity):
            own = part[r * experts : (r + 1) * experts, :]
            row = r * pieces + k
            scr[pl.ds(row, experts, stride=chunk_rows), :] = own[:, :LANE]
            scr[pl.ds(row + 1, experts, stride=chunk_rows), :] = own[:, LANE:]


def expert_hidden(x, gate, up):
    gate_value = jnp.dot(x, gate, preferred_element_type=f32)
    up_value = jnp.dot(x, up, preferred_element_type=f32)
    return (gate_value * jax.nn.sigmoid(gate_value) * up_value).astype(bf16)


def expert_first_body(
    capacity, chunk_rows, in_ref, g0, u0, g1, u1, g2, u2, d0, d1a, d1b, d2a, d2b, rows_ref, sum_ref, scr
):
    slots, width = rows_ref.shape
    pieces = width // LANE
    count = slots // capacity
    scr[...] = in_ref[...].astype(f32)
    for r in range(capacity):
        for k in range(pieces):
            got = scr[pl.ds(r * pieces + k, count, stride=chunk_rows), :]
            rows_ref[r * count : (r + 1) * count, k * LANE : (k + 1) * LANE] = got.astype(bf16)
    x = rows_ref[...]
    hidden = [expert_hidden(x, g[...], u[...]) for g, u in ((g0, u0), (g1, u1), (g2, u2))]
    for k in range(0, pieces, 2):
        cols = slice(k * LANE, (k + 2) * LANE)
        low_down = jnp.concatenate([d1a[:, cols], d1b[:, cols]], axis=0)
        high_down = jnp.concatenate([d2a[:, cols], d2b[:, cols]], axis=0)
        sum_ref[:, cols] = (
            jnp.dot(hidden[0], d0[:, cols], preferred_element_type=f32)
            + jnp.dot(hidden[1], low_down, preferred_element_type=f32)
            + jnp.dot(hidden[2], high_down, preferred_element_type=f32)
        )


def expert_hidden_body(rows_ref, g, u, hidden_ref):
    hidden_ref[...] = expert_hidden(rows_ref[...], g[...], u[...])


def expert_last_body(
    capacity, hidden_ref, sum_ref, da, db, out_ref, held_a, held_b, packed, scr, in_sems, out_sems
):
    slots, width = sum_ref.shape
    pieces = width // LANE
    parts = in_sems.shape[0] // 2
    span = width // parts
    arriving = []
    for i in range(parts):
        for j, (source, target) in enumerate(((da, held_a), (db, held_b))):
            cols = pl.ds(i * span, span)
            arriving.append(
                pltpu.make_async_copy(source.at[:, cols], target.at[:, cols], in_sems.at[2 * i + j])
            )
    for copy in arriving:
        copy.start()
    hidden = hidden_ref[...]
    sources = slots // capacity
    for k in range(0, pieces, 2):
        if k * LANE % span == 0:
            first = 2 * (k * LANE // span)
            arriving[first].wait()
            arriving[first + 1].wait()
        cols = slice(k * LANE, (k + 2) * LANE)
        part = sum_ref[:, cols] + jnp.dot(
            hidden,
            jnp.concatenate([held_a[:, cols], held_b[:, cols]], axis=0),
            preferred_element_type=f32,
        )
        for r in range(capacity):
            own = part[r * sources : (r + 1) * sources, :]
            row = r * pieces + k
            scr[pl.ds(row, sources, stride=capacity * pieces), :] = own[:, :LANE]
            scr[pl.ds(row + 1, sources, stride=capacity * pieces), :] = own[:, LANE:]
    count = out_sems.shape[0]
    chunk = packed.shape[0] // count
    leaving = []
    for i in range(count):
        packed[i * chunk : (i + 1) * chunk, :] = scr[i * chunk : (i + 1) * chunk, :].astype(bf16)
        rows = pl.ds(i * chunk, chunk)
        leaving.append(
            pltpu.make_async_copy(packed.at[rows, :], out_ref.at[rows, :], out_sems.at[i])
        )
        leaving[-1].start()
    for copy in leaving:
        copy.wait()


def shared_pack_body(core_ref, gate_ref, up_ref, down_ref, out_ref):
    width, chans = gate_ref.shape
    half = chans // 2
    core = core_ref[0]
    gate = gate_ref[...].astype(f32)
    up = up_ref[...].astype(f32)
    left = lax.broadcasted_iota(jnp.int32, (width, chans), 1) < half
    first = jnp.where(left, gate, pltpu.roll(up, half, 1))
    second = jnp.where(left, pltpu.roll(gate, half, 1), up)
    out_ref[:width, :] = jnp.where(core == 0, first, second).astype(bf16)
    rows = pl.multiple_of(core * half, half)
    for j in range(width // LANE):
        out_ref[width + j * half : width + (j + 1) * half, :] = down_ref[
            pl.ds(rows, half), j * LANE : (j + 1) * LANE
        ]


def shared_body(mine_ref, other_ref, own, low, high, far, sum_ref, send_ref):
    rows, width = mine_ref.shape
    x = jnp.concatenate([mine_ref[...], other_ref[...]], axis=0)
    lanes = lax.broadcasted_iota(jnp.int32, (2 * rows, LANE), 1) < LANE // 2
    packs = (own, low, high, far)
    hidden = []
    for pair in (packs[:2], packs[2:]):
        halves = []
        for pack in pair:
            both = jnp.dot(x, pack[:width, :], preferred_element_type=f32)
            up_value = pltpu.roll(both, LANE // 2, 1)
            halves.append(both * jax.nn.sigmoid(both) * up_value)
        hidden.append(jnp.where(lanes, halves[0], pltpu.roll(halves[1], LANE // 2, 1)))
    hidden = jnp.concatenate(hidden, axis=1).astype(bf16)
    units = LANE // 2
    for j in range(0, width // LANE, 2):
        down = jnp.concatenate(
            [
                jnp.concatenate(
                    [pack[width + i * units : width + (i + 1) * units, :] for pack in packs], axis=0
                )
                for i in (j, j + 1)
            ],
            axis=1,
        )
        part = jnp.dot(hidden, down, preferred_element_type=f32)
        cols = slice(j * LANE, (j + 2) * LANE)
        sum_ref[:, cols] = part[:rows]
        send_ref[:, cols] = part[rows:].astype(bf16)


def combine_body(capacity, experts, in_ref, routes_ref, scores_ref, shared_ref, out_ref, scr):
    rows, width = out_ref.shape
    pieces = width // LANE
    slots = experts * capacity
    scr[...] = in_ref[...].astype(f32)
    first = routes_ref[:, 0:1]
    second = routes_ref[:, 1:2]
    names = lax.broadcasted_iota(jnp.int32, (rows, experts), 1)
    hit0 = (names == first).astype(f32)
    hit1 = (names == second).astype(f32)
    earlier = (
        lax.broadcasted_iota(jnp.int32, (rows, rows), 1)
        < lax.broadcasted_iota(jnp.int32, (rows, rows), 0)
    ).astype(bf16)
    before = jnp.dot(earlier, (hit0 + hit1).astype(bf16), preferred_element_type=f32)
    slot0 = first * capacity + jnp.sum(before * hit0, axis=1, keepdims=True).astype(jnp.int32)
    slot1 = second * capacity + jnp.sum(before * hit1, axis=1, keepdims=True).astype(jnp.int32)
    place = lax.broadcasted_iota(jnp.int32, (rows, slots), 1)
    pick = jnp.concatenate(
        [(place == slot0).astype(bf16), (place == slot1).astype(bf16)], axis=0
    )
    scores = scores_ref[...].astype(f32)
    weights = scores / jnp.sum(scores, axis=1, keepdims=True) * route_scale
    w0 = weights[:, 0:1]
    w1 = weights[:, 1:2]
    for k in range(0, pieces, 2):
        both = jnp.concatenate(
            [
                scr[pl.ds(k, slots, stride=pieces), :].astype(bf16),
                scr[pl.ds(k + 1, slots, stride=pieces), :].astype(bf16),
            ],
            axis=1,
        )
        got = jnp.dot(pick, both, preferred_element_type=f32)
        cols = slice(k * LANE, (k + 2) * LANE)
        out_ref[:, cols] = (
            got[:rows] * w0 + got[rows:] * w1 + shared_ref[:, cols]
        ).astype(bf16)


def conv_silu(x_ref, tail, taps_ref, pad_ref):
    rows, chans = x_ref.shape
    taps = taps_ref.shape[0]
    start = 8 - taps + 1
    pad_ref[8 : 8 + rows, :chans] = x_ref[...].astype(f32)
    pad_ref[start:8, :chans] = tail.astype(f32)
    weights = taps_ref[...].astype(f32)
    total = weights[0:1, :] * pad_ref[start : start + rows, :chans]
    for j in range(1, taps):
        total = total + weights[j : j + 1, :] * pad_ref[start + j : start + j + rows, :chans]
    return total * jax.nn.sigmoid(total)


def precise(a, b, contract=(1, 0)):
    return lax.dot_general(
        a,
        b,
        (((contract[0],), (contract[1],)), ((), ())),
        precision=highest,
        preferred_element_type=f32,
    )


def keep_near(value):
    return pltpu.with_memory_space_constraint(value, pltpu.VMEM)


def spread(heads, chans):
    head = lax.broadcasted_iota(jnp.int32, (heads, chans), 0)
    chan = lax.broadcasted_iota(jnp.int32, (heads, chans), 1)
    return (chan // (chans // heads) == head).astype(f32)


def front_body(capacity, experts, chunk_rows, *refs):
    inputs, refs = refs[:13], refs[13:]
    outputs, refs = refs[:5], refs[5:]
    held_in, refs = refs[:13], refs[13:]
    held_out, refs = refs[:5], refs[5:]
    scr, pad_ref, values_ref, in_sems, out_sems = refs
    arriving = [
        pltpu.make_async_copy(source, target, in_sems.at[i])
        for i, (source, target) in enumerate(zip(inputs, held_in))
    ]
    leaving = [
        pltpu.make_async_copy(source, target, out_sems.at[i])
        for i, (source, target) in enumerate(zip(held_out, outputs))
    ]
    for copy in arriving:
        copy.start()
    x_ref, gain_ref, routes_ref, heads_ref, write_ref, read_ref, tail_ref = held_in[:7]
    pre_ref, extra_ref, rate_ref, head_taps, write_taps, read_taps = held_in[7:]
    normed_ref, out_ref, local_ref, read_out, grow_out = held_out
    for copy in arriving[:3]:
        copy.wait()
    place_rows(capacity, experts, chunk_rows, x_ref, gain_ref, routes_ref, normed_ref, scr)
    leaving[0].start()
    for copy in arriving[3:]:
        copy.wait()
    rows, chans = heads_ref.shape
    heads = pre_ref.shape[0]
    tail = tail_ref[...]
    values_ref[...] = conv_silu(heads_ref, tail[:, :chans], head_taps, pad_ref)
    write = conv_silu(write_ref, tail[:, chans : chans + STATE], write_taps, pad_ref)
    read = conv_silu(read_ref, tail[:, chans + STATE :], read_taps, pad_ref)
    read_out[...] = read
    pre = pre_ref[...]
    step = jnp.maximum(pre, 0.0) + jnp.log1p(jnp.exp(-jnp.abs(pre)))
    heads_across = lax.broadcasted_iota(jnp.int32, (heads, heads), 1)
    heads_down = lax.broadcasted_iota(jnp.int32, (heads, heads), 0)
    rate = jnp.sum(
        jnp.where(heads_across == heads_down, jnp.exp(rate_ref[...]), 0.0), axis=1, keepdims=True
    )
    log_rate = -rate * step + extra_ref[...]
    row = lax.broadcasted_iota(jnp.int32, (rows, rows), 0)
    col = lax.broadcasted_iota(jnp.int32, (rows, rows), 1)
    lower = row >= col
    cum = precise(log_rate, (row <= col).astype(f32))
    cum_down = precise(lower.astype(f32), log_rate, (1, 1))
    step_down = precise((row == col).astype(f32), step, (1, 1))
    grow_out[...] = jnp.exp(cum_down)
    wide = spread(heads, chans)
    to_end = step_down * jnp.exp(cum_down[rows - 1 : rows, :] - cum_down)
    ending = values_ref[...] * precise(to_end, wide)
    state = precise(ending, write, (0, 0))
    chunks = experts
    base = chunk_rows - 24
    repeat = chunks // heads
    chunk = lax.broadcasted_iota(jnp.int32, (chunks, heads), 0)
    head = lax.broadcasted_iota(jnp.int32, (chunks, heads), 1)
    total = precise((chunk // repeat == head).astype(f32), cum)[:, rows - 1 : rows]
    top = total.astype(bf16).astype(f32)
    middle = (total - top).astype(bf16).astype(f32)
    bottom = total - top - middle
    lane = lax.broadcasted_iota(jnp.int32, (chunks, STATE), 1)
    decays = jnp.where(
        lane == 0, top, jnp.where(lane == 1, middle, jnp.where(lane == 2, bottom, 0.0))
    )
    for j in range(chunks):
        row = chunk_rows * j + base
        scr[row : row + 16, :] = state[16 * j : 16 * j + 16, :]
        scr[row + 16 : row + 24, :] = jnp.broadcast_to(decays[j : j + 1, :], (8, STATE))
    out_ref[...] = scr[...].astype(bf16)
    leaving[1].start()
    affinity = precise(read, write, (1, 1))
    left = lax.broadcasted_iota(jnp.int32, (rows, LANE), 1) < HEAD_DIM
    for pair in range(heads // 2):
        mixed = []
        for e in (2 * pair, 2 * pair + 1):
            gap = cum_down[:, e : e + 1] - cum[e : e + 1, :]
            within = jnp.exp(jnp.where(lower, gap, -jnp.inf))
            mixed.append(affinity * within * step[e : e + 1, :])
        cols = slice(pair * LANE, (pair + 1) * LANE)
        part = precise(jnp.concatenate(mixed, axis=0), values_ref[:, cols])
        local_ref[:, cols] = jnp.where(left, part[:rows], part[rows:])
    for copy in leaving[2:]:
        copy.start()
    for copy in leaving:
        copy.wait()


def carry_body(in_ref, out_ref, scr, sums):
    chunks = in_ref.shape[0]
    scr[...] = in_ref[...].astype(f32).reshape(scr.shape)
    lane = lax.broadcasted_iota(jnp.int32, (chunks, STATE), 1)
    pieces = scr[pl.ds(16, chunks, stride=24), :]
    decay = jnp.sum(jnp.where(lane < 3, pieces, 0.0), axis=1, keepdims=True)
    row = lax.broadcasted_iota(jnp.int32, (chunks, chunks), 0)
    col = lax.broadcasted_iota(jnp.int32, (chunks, chunks), 1)
    held = jnp.broadcast_to(decay, (chunks, STATE))
    ends = precise((row >= col).astype(f32), held)[:, :chunks]
    ends_across = precise(held, (row <= col).astype(f32), (0, 0))[0:1, :]
    carry = jnp.exp(jnp.where(row > col, ends - decay - ends_across, -jnp.inf))
    for r in range(0, 16, 2):
        both = jnp.concatenate(
            [
                scr[pl.ds(r, chunks, stride=24), :],
                scr[pl.ds(r + 1, chunks, stride=24), :],
            ],
            axis=1,
        )
        part = precise(carry, both)
        sums[pl.ds(r, chunks, stride=16), :] = part[:, :STATE]
        sums[pl.ds(r + 1, chunks, stride=16), :] = part[:, STATE:]
    out_ref[...] = sums[...].astype(bf16)


def mixer_out_body(
    place_ref, state_ref, read_ref, grow_ref, local_ref, gate_ref, gain_ref, weight_ref, *refs
):
    outs = refs[:-2]
    normed_ref, total_ref = refs[-2:]
    rows, chans = local_ref.shape
    heads = grow_ref.shape[1]
    carried = precise(read_ref[...], state_ref[...].astype(f32), (1, 1))
    scan_out = local_ref[...] + carried * precise(grow_ref[...], spread(heads, chans))
    gate = gate_ref[...].astype(f32)
    gated = scan_out * (gate * jax.nn.sigmoid(gate))
    gated = gated * lax.rsqrt(jnp.mean(gated * gated, axis=-1, keepdims=True) + eps_norm)
    normed_ref[...] = (gated * gain_ref[...]).astype(bf16)
    total_ref[...] = jnp.dot(normed_ref[...], weight_ref[...], preferred_element_type=f32)
    parts = len(outs)
    block = rows // parts
    for by, out in enumerate(outs):
        target = lax.rem(place_ref[0] + by, parts)
        out[...] = total_ref[pl.ds(pl.multiple_of(target * block, block), block), :].astype(bf16)


def layer(
    head_inputs_unfiltered,
    group_write_vectors,
    group_read_vectors,
    output_gate_inputs,
    step_preactivation,
    extra_decay_logs,
    head_decay_logs,
    head_filter_taps,
    write_filter_taps,
    read_filter_taps,
    grouped_norm_gain,
    mixer_output_weight,
    expert_input_rows,
    expert_norm_gain,
    routes,
    router_chosen_scores,
    routed_gate_weight,
    routed_up_weight,
    routed_down_weight,
    shared_gate_weight,
    shared_up_weight,
    shared_down_weight,
):
    tp_count = lax.axis_size("tp")
    tp_index = lax.axis_index("tp")
    ep_count = lax.axis_size(EP)
    core = lax.axis_index("ep_2")
    rows, width = expert_input_rows.shape
    experts = routed_gate_weight.shape[0] * ep_count
    capacity = 3 * rows * routes.shape[1] // (2 * experts)
    slots = experts * capacity
    pieces = width // LANE
    exchanged = (experts, capacity * pieces, LANE)

    mix_rows, head_chans = head_inputs_unfiltered.shape
    taps = head_filter_taps.shape[0]
    tail_rows = jnp.concatenate(
        [
            head_inputs_unfiltered[mix_rows - taps + 1 :],
            group_write_vectors[mix_rows - taps + 1 :],
            group_read_vectors[mix_rows - taps + 1 :],
        ],
        axis=1,
    )
    tail_rows = shift(tail_rows, EP, 1, False)
    gate, up, down = routed_gate_weight[0], routed_up_weight[0], routed_down_weight[0]
    low_gate = shift(gate, "tp", 1, True)
    high_gate = shift(gate, "tp", -1, True)
    low_up = shift(up, "tp", 1, True)
    high_up = shift(up, "tp", -1, True)

    heads = step_preactivation.shape[0]
    chunk_rows = capacity * pieces + 24
    front_in = (
        expert_input_rows,
        expert_norm_gain[None, :],
        routes.T,
        head_inputs_unfiltered,
        group_write_vectors,
        group_read_vectors,
        tail_rows,
        step_preactivation,
        extra_decay_logs,
        head_decay_logs[None, :],
        head_filter_taps,
        write_filter_taps,
        read_filter_taps,
    )
    front_out = (
        pltpu.HBM((rows, width), bf16),
        pltpu.HBM((experts * chunk_rows, LANE), bf16),
        pltpu.HBM((mix_rows, head_chans), f32),
        pltpu.HBM((mix_rows, STATE), f32),
        pltpu.HBM((mix_rows, heads), f32),
    )
    in_hbm = pl.BlockSpec(memory_space=pltpu.HBM)
    normed, sent, local_part, read_values, growth = pl.pallas_call(
        functools.partial(front_body, capacity, experts, chunk_rows),
        out_shape=front_out,
        in_specs=[in_hbm] * len(front_in),
        out_specs=(in_hbm,) * len(front_out),
        scratch_shapes=[pltpu.VMEM(v.shape, v.dtype) for v in front_in + front_out]
        + [
            pltpu.VMEM((experts * chunk_rows, LANE), f32),
            pltpu.VMEM((mix_rows + 8, head_chans), f32),
            pltpu.VMEM((mix_rows, head_chans), f32),
            pltpu.SemaphoreType.DMA((len(front_in),)),
            pltpu.SemaphoreType.DMA((len(front_out),)),
        ],
        compiler_params=pltpu.CompilerParams(vmem_limit_bytes=24 * MIB),
        name="front",
    )(*(pltpu.with_memory_space_constraint(v, pltpu.HBM) for v in front_in))
    arrived = lax.all_to_all(
        sent.reshape(experts, chunk_rows, LANE), EP, 0, 0, tiled=True
    )
    half = down.shape[0] // 2
    down_a, down_b = down[:half], down[half:]
    low_down_a = shift(down_a, "tp", 1, True)
    high_down_b = shift(down_b, "tp", -1, True)
    low_down_b = shift(down_b, "tp", 1, True)
    high_down_a = shift(down_a, "tp", -1, True)
    partner = shift(normed, "ep_2", 1, True)
    far_gate = shift(low_gate, "tp", 1, True)
    far_up = shift(high_up, "tp", -1, True)
    far_down_a = shift(low_down_a, "tp", 1, True)
    far_down_b = shift(high_down_b, "tp", -1, True)
    entering = pl.pallas_call(
        carry_body,
        out_shape=jax.ShapeDtypeStruct((ep_count * 16, STATE), bf16),
        grid=(1,),
        in_specs=[
            pl.BlockSpec((ep_count, 24, STATE), lambda i: (0, capacity * pieces // 24, 0))
        ],
        out_specs=pl.BlockSpec((ep_count * 16, STATE), lambda i: (0, 0)),
        scratch_shapes=[
            pltpu.VMEM((ep_count * 24, STATE), f32),
            pltpu.VMEM((ep_count * 16, STATE), f32),
        ],
        compiler_params=pltpu.CompilerParams(vmem_limit_bytes=8 * MIB),
        name="carry",
    )(arrived)
    entering = lax.all_to_all(entering.reshape(ep_count, 16, STATE), EP, 0, 0, tiled=True)

    low_gate, low_up, low_down_a, low_down_b = map(
        keep_near, (low_gate, low_up, low_down_a, low_down_b)
    )
    high_gate, high_up, high_down_a, high_down_b = map(
        keep_near, (high_gate, high_up, high_down_a, high_down_b)
    )
    far_gate, far_up = map(keep_near, (far_gate, far_up))
    expert_rows, expert_sum = call(
        functools.partial(expert_first_body, capacity, chunk_rows),
        (pltpu.VMEM((slots, width), bf16), pltpu.VMEM((slots, width), f32)),
        [pltpu.VMEM((experts * chunk_rows, LANE), f32)],
        16,
    )(
        arrived.reshape(experts * chunk_rows, LANE),
        gate,
        up,
        low_gate,
        low_up,
        high_gate,
        high_up,
        down,
        low_down_a,
        low_down_b,
        high_down_a,
        high_down_b,
    )
    far_hidden = call(
        expert_hidden_body, jax.ShapeDtypeStruct((slots, down.shape[0]), bf16), (), 10
    )(expert_rows, far_gate, far_up)
    in_vmem = pl.BlockSpec(memory_space=pltpu.VMEM)
    sent_back = pl.pallas_call(
        functools.partial(expert_last_body, capacity),
        out_shape=pltpu.HBM((slots * pieces, LANE), bf16),
        in_specs=[in_vmem, in_vmem, in_hbm, in_hbm],
        out_specs=in_hbm,
        scratch_shapes=[
            pltpu.VMEM((half, width), bf16),
            pltpu.VMEM((half, width), bf16),
            pltpu.VMEM((slots * pieces, LANE), bf16),
            pltpu.VMEM((slots * pieces, LANE), f32),
            pltpu.SemaphoreType.DMA((8,)),
            pltpu.SemaphoreType.DMA((4,)),
        ],
        compiler_params=pltpu.CompilerParams(vmem_limit_bytes=16 * MIB),
        name="experts_last",
    )(far_hidden, expert_sum, far_down_a, far_down_b)
    returned = lax.all_to_all(sent_back.reshape(exchanged), EP, 0, 0, tiled=True)

    block = mix_rows // tp_count
    mix_parts = pl.pallas_call(
        mixer_out_body,
        out_shape=[jax.ShapeDtypeStruct((block, width), bf16)] * tp_count,
        in_specs=[pl.BlockSpec(memory_space=pltpu.SMEM)]
        + [pl.BlockSpec(memory_space=pltpu.VMEM)] * 7,
        scratch_shapes=[
            pltpu.VMEM((mix_rows, head_chans), bf16),
            pltpu.VMEM((mix_rows, width), f32),
        ],
        compiler_params=pltpu.CompilerParams(vmem_limit_bytes=20 * MIB),
        name="mixer_out",
    )(
        tp_index[None].astype(jnp.int32),
        entering.reshape(ep_count * 16, STATE),
        read_values,
        growth,
        local_part,
        output_gate_inputs,
        grouped_norm_gain[None, :],
        mixer_output_weight,
    )
    mix_parts = [shift(part, "tp", by, True) if by else part for by, part in enumerate(mix_parts)]
    mixer_result = sum(part.astype(f32) for part in mix_parts).astype(bf16)

    units = shared_down_weight.shape[0] // 2
    shared_own = pl.pallas_call(
        shared_pack_body,
        out_shape=jax.ShapeDtypeStruct((width + pieces * units, LANE), bf16),
        in_specs=[pl.BlockSpec(memory_space=pltpu.SMEM)]
        + [pl.BlockSpec(memory_space=pltpu.VMEM)] * 3,
        compiler_params=pltpu.CompilerParams(vmem_limit_bytes=8 * MIB),
        name="shared_pack",
    )(
        core[None].astype(jnp.int32),
        shared_gate_weight,
        shared_up_weight,
        shared_down_weight,
    )
    shared_low = shift(shared_own, "tp", 1, True)
    shared_high = shift(shared_own, "tp", -1, True)
    shared_far = shift(shared_low, "tp", 1, True)
    shared_sum, shared_send = call(
        shared_body,
        (
            pltpu.HBM((rows, width), f32),
            jax.ShapeDtypeStruct((rows, width), bf16),
        ),
        (),
        16,
    )(normed, partner, shared_own, shared_low, shared_high, shared_far)
    shared_got = shift(shared_send, "ep_2", 1, True)

    moe_result = call(
        functools.partial(combine_body, capacity, experts),
        jax.ShapeDtypeStruct((rows, width), bf16),
        [pltpu.VMEM((slots * pieces, LANE), f32)],
        16,
    )(
        returned.reshape(slots * pieces, LANE),
        routes,
        router_chosen_scores,
        shared_sum + shared_got.astype(f32),
    )
    return (mixer_result, moe_result)


def solution(mesh):
    split = Mesh(mesh.devices.reshape(8, 4, 2, mesh.shape["tp"]), ("ep_0", "ep_1", "ep_2", "tp"))
    placed = (
        P(EP, "tp"),
        P(EP, "tp"),
        P(EP, "tp"),
        P(EP, "tp"),
        P("tp", EP),
        P("tp", EP),
        P("tp"),
        P(None, "tp"),
        P(None, "tp"),
        P(None, "tp"),
        P("tp"),
        P("tp", None),
        P(EP_TP, None),
        P(),
        P(EP_TP, None),
        P(EP_TP, None),
        P(EP, None, "tp"),
        P(EP, None, "tp"),
        P(EP, "tp", None),
        P(None, "tp"),
        P(None, "tp"),
        P("tp", None),
    )
    return jax.shard_map(
        layer,
        mesh=split,
        in_specs=placed,
        out_specs=(P(EP_TP, None), P(EP_TP, None)),
        check_vma=False,
    )
```
